32 devices in a mesh: sp: 8 (over z, x), tp: 4 (over y, core).
Axes of the slice: x: 2, y: 2, z: 4, core: 2. Of those that a mesh axis runs over, the one named last changes fastest.
Arguments:
- query_nope: bfloat16 [2048, 1024], P('sp', 'tp'), may hold values from -24 to 24
- query_rope: bfloat16 [2048, 512], P('sp', 'tp'), may hold values from -384 to 384
- latent: bfloat16 [2048, 256], P('sp'), may hold values from -6 to 6
- key_rope: bfloat16 [2048, 64], P('sp'), may hold values from -8 to 8
- latent_gain: bfloat16 [256], replicated, may hold values from 0.099609375 to 1.8984375
- key_up: bfloat16 [256, 1024], replicated, may hold values from -0.375 to 0.375
- value_up: bfloat16 [256, 1024], replicated, may hold values from -0.375 to 0.375
- out_proj: bfloat16 [1024, 2048], P('tp'), may hold values from -0.1875 to 0.1875
- residual: bfloat16 [2048, 2048], P(('sp', 'tp')), may hold values from -6 to 6
- ffn_gain: bfloat16 [2048], replicated, may hold values from 0.099609375 to 1.8984375
- expert_ids: int32 [2048, 4], P(('sp', 'tp')), may hold values from 0 to 7, all different within a row; in each aligned block of 64 rows (0 to 63, 64 to 127, ...) at most 64 rows name the same one
- route_weights: float32 [2048, 4], P(('sp', 'tp')), may hold values from 0.1 to 1
- expert_gate: bfloat16 [8, 2048, 384], P('sp'), may hold values from -0.125 to 0.125
- expert_up: bfloat16 [8, 2048, 384], P('sp'), may hold values from -0.125 to 0.125
- expert_down: bfloat16 [8, 384, 2048], P('sp'), may hold values from -0.3125 to 0.3125
- shared_gate: bfloat16 [2048, 384], replicated, may hold values from -0.125 to 0.125
- shared_up: bfloat16 [2048, 384], replicated, may hold values from -0.125 to 0.125
- shared_down: bfloat16 [384, 2048], replicated, may hold values from -0.3125 to 0.3125
Outputs:
- layer_out: bfloat16 [2048, 2048], P(('sp', 'tp'))
The draws below stay inside these ranges and needn't reach their ends.
Inputs may be any that keep to these rules, and one draw needn't show every extreme that they name: `expert_ids`: each row names 4 different experts; among the 64 rows of one aligned block no expert is named by more than 64 rows.
All inputs are finite; a program needn't handle non-finite values.
Results may differ from the reference program's by a relative error of at most 0.017.
Values may be sent and summed in bfloat16 or wider, within the bound.
A program may use at most 128 MiB of HBM per device.

```python
import math
import jax
import jax.numpy as jnp
import numpy as np
from jax import lax

D = 2048
HEADS = 8
NOPE = 128
ROPE = 64
VDIM = 128
KV_RANK = 256
FF = 384
TOP = 4
EXPERTS = 8
SEQ = 2048
TOK_DEV = 64
CAP = 64
N_TP = 4


def draw_query_nope(key, part):
    own_key = jax.random.fold_in(key, 1)
    base_draw = 4.0 * jax.random.truncated_normal(own_key, -6.0, 6.0, (SEQ, HEADS * NOPE), jnp.float32)
    return base_draw.astype(jnp.bfloat16)


def draw_query_rope(key, part):
    own_key = jax.random.fold_in(key, 2)
    base_draw = 4.0 * jax.random.truncated_normal(own_key, -6.0, 6.0, (SEQ, HEADS * ROPE), jnp.float32)
    return base_draw.astype(jnp.bfloat16)


def draw_key_rope(key, part):
    own_key = jax.random.fold_in(key, 3)
    base_draw = jax.random.truncated_normal(own_key, -6.0, 6.0, (SEQ, ROPE), jnp.float32)
    return base_draw.astype(jnp.bfloat16)


def shard_levels(stream_key, dims, cuts, smallest, high):
    def one(dim, blocks):
        heights = jax.random.uniform(jax.random.fold_in(jax.random.fold_in(stream_key, 6), dim), (blocks,), jnp.float32, smallest / len(cuts), high / len(cuts))
        return jnp.repeat(jnp.exp(heights), dims[dim] // blocks).reshape((-1,) + (1,) * (len(dims) - dim - 1))

    level = one(*cuts[0])
    for cut in cuts[1:]:
        level = level * one(*cut)
    return level


def shared_out(key, own, number, rows, count, top, limit, skew):
    order = jax.random.permutation(key, count)
    crowded, ordinary = portions_of(count, rows * top, limit, skew, True), portions_of(count, rows * top, limit, skew, False)
    places = jnp.arange(count)

    def named(tallies, rotation):
        used = int((tallies > 0).sum())
        fixed = max(1, used // 4)
        moved = fixed + (places - fixed + rotation * (used - fixed)) % max(1, count - fixed)
        return jnp.zeros((count,), jnp.int32).at[order[jnp.where(places < fixed, places, moved)]].set(jnp.asarray(tallies, jnp.int32))

    tallies = jnp.where(number % 4 == 0, named(crowded, number // 4), named(ordinary, number - number // 4 - 1))
    mixed = jax.random.permutation(jax.random.fold_in(own, 3), count)
    donor, sink = mixed[0:count // 2 * 2:2], mixed[1:count // 2 * 2:2]
    slack = jnp.minimum(tallies[donor] - 1, limit - tallies[sink]) // 2
    slack = jnp.where((donor == order[0]) | (sink == order[0]) | (tallies[sink] == 0), 0, jnp.maximum(slack, 0))
    moved = jax.random.randint(jax.random.fold_in(own, 4), (count // 2,), 0, 1 << 20) % (slack + 1)
    tallies = tallies.at[donor].add(-moved).at[sink].add(moved)
    labels = jnp.searchsorted(jnp.cumsum(tallies), jnp.arange(rows * top), side="right").astype(jnp.int32)
    grid = labels.reshape(top, rows).T
    grid = grid[jax.random.permutation(jax.random.fold_in(own, 1), rows)]
    rotation = jax.random.randint(jax.random.fold_in(own, 2), (rows, 1), 0, top)
    return jnp.take_along_axis(grid, (jnp.arange(top)[None, :] + rotation) % top, axis=1)


def portions_of(number_of, total, limit, lean, full):
    loads = [(1 << 20) // math.isqrt(standing ** lean) + 1 for standing in range(1, number_of + 1)]
    largest = limit if full else min(limit, max(-(-total // number_of), total * loads[0] // sum(loads)))
    least = 1 if total - largest >= number_of - 1 else 0
    holding, spare = [largest] + [least] * (number_of - 1), total - largest - least * (number_of - 1)
    while spare > 0:
        movable = [i for i in range(1, number_of) if holding[i] < largest] or [i for i in range(1, number_of) if holding[i] < limit]
        mass, remaining = sum([loads[i] for i in movable]), spare
        for i in movable:
            more = min(limit - holding[i], max(1, remaining * loads[i] // mass), spare)
            holding[i] = holding[i] + more
            spare = spare - more
    return np.array(holding)


def scatter_about(key, shape, width, bound, shards=(), kind=jnp.bfloat16):
    factor_of = shard_levels(key, shape, shards, -0.22, 0.18) if shards else 1.0
    values = jax.random.normal(key, shape, jnp.float32) * width * factor_of
    return jnp.minimum(jnp.maximum(values, -bound), bound).astype(kind)


def setup_inputs(seed: int = 0) -> dict:
    keys = jax.random.split(jax.random.key(seed), 19)
    query_nope = draw_query_nope(jax.random.fold_in(keys[18], 71), 0)
    query_rope = draw_query_rope(jax.random.fold_in(keys[18], 71), 0)
    latent = scatter_about(keys[2], (SEQ, KV_RANK), 1.0, 6.0, ((0, 8),))
    key_rope = draw_key_rope(jax.random.fold_in(keys[18], 71), 0)
    latent_gain = jnp.clip(1.0 + 0.18 * jax.random.normal(keys[4], (KV_RANK,), jnp.float32), 0.099609375, 1.8984375).astype(jnp.bfloat16)
    key_up = scatter_about(keys[5], (KV_RANK, HEADS * NOPE), KV_RANK ** -0.5, 0.375)
    value_up = scatter_about(keys[6], (KV_RANK, HEADS * VDIM), KV_RANK ** -0.5, 0.375)
    out_proj = scatter_about(keys[7], (HEADS * VDIM, D), (HEADS * VDIM) ** -0.5, 0.1875, ((0, 4),))
    residual = scatter_about(keys[8], (SEQ, D), 1.0, 6.0, ((0, 32),))
    ffn_gain = jnp.clip(1.0 + 0.18 * jax.random.normal(keys[9], (D,), jnp.float32), 0.099609375, 1.8984375).astype(jnp.bfloat16)
    expert_ids_keys = jax.random.split(jax.random.fold_in(keys[10], 1), SEQ // TOK_DEV)
    expert_ids_turns = jax.random.permutation(jax.random.fold_in(keys[10], 3), SEQ // TOK_DEV)
    expert_ids = jax.vmap(lambda own, number: shared_out(jax.random.fold_in(keys[10], 2), own, number, TOK_DEV, EXPERTS, TOP, CAP, 1))(expert_ids_keys, expert_ids_turns).reshape((SEQ, TOP))
    route_weights = jnp.clip(jnp.exp(math.log(1.0) - 2.3025851 * jax.random.uniform(keys[11], (SEQ, TOP), jnp.float32) ** shard_levels(keys[11], (SEQ, TOP), ((0, 32),), -0.2, 0.2)), 0.1, 1.0)
    expert_gate = scatter_about(keys[12], (EXPERTS, D, FF), D ** -0.5, 0.125, ((0, 8),))
    expert_up = scatter_about(keys[13], (EXPERTS, D, FF), D ** -0.5, 0.125, ((0, 8),))
    expert_down = scatter_about(keys[14], (EXPERTS, FF, D), FF ** -0.5, 0.3125, ((0, 8),))
    shared_gate = scatter_about(keys[15], (D, FF), D ** -0.5, 0.125)
    shared_up = scatter_about(keys[16], (D, FF), D ** -0.5, 0.125)
    shared_down = scatter_about(keys[17], (FF, D), FF ** -0.5, 0.3125)
    return {"query_nope": query_nope, "query_rope": query_rope, "latent": latent, "key_rope": key_rope, "latent_gain": latent_gain, "key_up": key_up, "value_up": value_up, "out_proj": out_proj, "residual": residual, "ffn_gain": ffn_gain, "expert_ids": expert_ids, "route_weights": route_weights, "expert_gate": expert_gate, "expert_up": expert_up, "expert_down": expert_down, "shared_gate": shared_gate, "shared_up": shared_up, "shared_down": shared_down}


rope_base = 10000.0
norm_eps = 1e-06

def scale_rows(values, gain_vec):
    as_float = values.astype(jnp.float32)
    factor = lax.rsqrt(lax.optimization_barrier(jnp.mean(as_float * as_float, axis=-1, keepdims=True)) + norm_eps)
    return (as_float * factor * gain_vec.astype(jnp.float32)).astype(jnp.bfloat16)

def rotate(values, positions):
    half_dim = values.shape[-1] // 2
    frequency = rope_base ** (-jnp.arange(half_dim, dtype=jnp.float32) / half_dim)
    angles = positions.astype(jnp.float32)[:, None, None] * frequency
    cosine = jnp.cos(angles)
    sine_part = jnp.sin(angles)
    as_float = values.astype(jnp.float32)
    first_half = as_float[..., :half_dim]
    second_half = as_float[..., half_dim:]
    return jnp.concatenate([first_half * cosine - second_half * sine_part, first_half * sine_part + second_half * cosine], axis=-1).astype(jnp.bfloat16)

def reference(query_nope, query_rope, latent, key_rope, latent_gain, key_up, value_up, out_proj, residual, ffn_gain, expert_ids, route_weights, expert_gate, expert_up, expert_down, shared_gate, shared_up, shared_down):
    length = latent.shape[0]
    model_width = residual.shape[1]
    positions = jnp.arange(length, dtype=jnp.int32)
    normed_latent = scale_rows(latent, latent_gain)
    keys_nope = jnp.dot(normed_latent, key_up, preferred_element_type=jnp.float32).astype(jnp.bfloat16)
    values = jnp.dot(normed_latent, value_up, preferred_element_type=jnp.float32).astype(jnp.bfloat16)
    key_heads = keys_nope.reshape(length, HEADS, NOPE).astype(jnp.float32)
    value_heads = values.reshape(length, HEADS, VDIM).astype(jnp.float32)
    rot_key = rotate(key_rope[:, None, :], positions)[:, 0, :].astype(jnp.float32)
    queries_nope = query_nope.reshape(length, HEADS, NOPE)
    rot_query = rotate(query_rope.reshape(length, HEADS, ROPE), positions)
    block_len = math.gcd(length, 512)
    score_scale = 1.0 / math.sqrt(NOPE + ROPE)

    def one_block(block_start):
        query_part = lax.dynamic_slice_in_dim(queries_nope, block_start, block_len, 0).astype(jnp.float32)
        rotary_part = lax.dynamic_slice_in_dim(rot_query, block_start, block_len, 0).astype(jnp.float32)
        scores = jnp.einsum('qhd,khd->hqk', query_part, key_heads)
        scores = (scores + jnp.einsum('qhd,kd->hqk', rotary_part, rot_key)) * score_scale
        query_pos = block_start + jnp.arange(block_len, dtype=jnp.int32)
        allowed = (positions[None, :] <= query_pos[:, None])[None]
        scores = jnp.where(allowed, scores, -1e+30)
        highest = lax.optimization_barrier(jnp.max(scores, axis=-1, keepdims=True))
        weights = jnp.where(allowed, jnp.exp(scores - highest), 0.0)
        denominators = lax.optimization_barrier(jnp.sum(weights, axis=-1))
        rounded_weights = lax.optimization_barrier(weights.astype(jnp.bfloat16))
        mixed = jnp.einsum('hqk,khd->qhd', rounded_weights.astype(jnp.float32), value_heads)
        return (mixed / denominators.T[:, :, None]).astype(jnp.bfloat16)
    starts = jnp.arange(length // block_len, dtype=jnp.int32) * block_len
    heads_out = lax.map(one_block, starts).reshape(length, HEADS * VDIM)
    group_width = HEADS * VDIM // N_TP
    attn_sum = jnp.zeros((length, model_width), jnp.float32)
    for group_index in range(N_TP):
        partial_rows = jnp.dot(heads_out[:, group_index * group_width:(group_index + 1) * group_width], out_proj[group_index * group_width:(group_index + 1) * group_width], preferred_element_type=jnp.float32)
        rounded_rows = lax.optimization_barrier(partial_rows.astype(jnp.bfloat16))
        attn_sum = attn_sum + rounded_rows.astype(jnp.float32)
    hidden_one = (residual.astype(jnp.float32) + attn_sum).astype(jnp.bfloat16)
    normed = scale_rows(hidden_one, ffn_gain)
    row_total = length * TOP
    flat_ids = expert_ids.reshape(-1).astype(jnp.int32)
    onehot = (flat_ids[:, None] == jnp.arange(EXPERTS, dtype=jnp.int32)[None, :]).astype(jnp.int32)
    slot_rank = lax.optimization_barrier(jnp.sum(jnp.cumsum(onehot, axis=0) * onehot, axis=1)) - 1
    most_rows = length // TOK_DEV * CAP
    target = (flat_ids * most_rows + slot_rank).astype(jnp.int32)
    slot_token = jnp.full((EXPERTS * most_rows,), length, jnp.int32).at[target].set(jnp.arange(row_total, dtype=jnp.int32) // TOP)
    slot_weight = jnp.zeros((EXPERTS * most_rows,), jnp.float32).at[target].set(route_weights.reshape(-1).astype(jnp.float32))
    padded = jnp.concatenate([normed, jnp.zeros((1, model_width), jnp.bfloat16)], axis=0)

    def one_expert(accum, expert_index):
        picks = lax.dynamic_slice_in_dim(slot_token, expert_index * most_rows, most_rows, 0)
        chosen = padded[picks]
        gate_part = jnp.dot(chosen, expert_gate[expert_index], preferred_element_type=jnp.float32)
        upper_part = jnp.dot(chosen, expert_up[expert_index], preferred_element_type=jnp.float32)
        expert_hidden = (jax.nn.silu(gate_part) * upper_part).astype(jnp.bfloat16)
        expert_rows = jnp.dot(expert_hidden, expert_down[expert_index], preferred_element_type=jnp.float32).astype(jnp.bfloat16)
        scaled = expert_rows.astype(jnp.float32) * lax.dynamic_slice_in_dim(slot_weight, expert_index * most_rows, most_rows, 0)[:, None]
        return (accum.at[picks].add(scaled), expert_index)
    accum = lax.scan(one_expert, jnp.zeros((length + 1, model_width), jnp.float32), jnp.arange(EXPERTS, dtype=jnp.int32))[0]
    routed = accum[:length].astype(jnp.bfloat16)
    shared_gate_part = jnp.dot(normed, shared_gate, preferred_element_type=jnp.float32)
    shared_upper = jnp.dot(normed, shared_up, preferred_element_type=jnp.float32)
    shared_hidden = (jax.nn.silu(shared_gate_part) * shared_upper).astype(jnp.bfloat16)
    shared_rows = jnp.dot(shared_hidden, shared_down, preferred_element_type=jnp.float32).astype(jnp.bfloat16)
    return (hidden_one.astype(jnp.float32) + routed.astype(jnp.float32) + shared_rows.astype(jnp.float32)).astype(jnp.bfloat16)
```

```python
import functools
import math

import jax
import jax.numpy as jnp
from jax import lax
from jax.experimental import pallas as pl
from jax.experimental.pallas import tpu as pltpu
from jax.sharding import PartitionSpec as P

NOPE = 128
ROPE = 64
VDIM = 128


rope_base = 10000.0
norm_eps = 1e-06


def scale_rows(values, gain_vec):
    as_float = values.astype(jnp.float32)
    factor = lax.rsqrt(jnp.mean(as_float * as_float, axis=-1, keepdims=True) + norm_eps)
    return (as_float * factor * gain_vec.astype(jnp.float32)).astype(jnp.bfloat16)


def rotate(values, positions):
    half_dim = values.shape[-1] // 2
    frequency = rope_base ** (-jnp.arange(half_dim, dtype=jnp.float32) / half_dim)
    angles = positions.astype(jnp.float32)[:, None, None] * frequency
    cosine = jnp.cos(angles)
    sine_part = jnp.sin(angles)
    as_float = values.astype(jnp.float32)
    first_half = as_float[..., :half_dim]
    second_half = as_float[..., half_dim:]
    return jnp.concatenate(
        [
            first_half * cosine - second_half * sine_part,
            first_half * sine_part + second_half * cosine,
        ],
        axis=-1,
    ).astype(jnp.bfloat16)


def start_body(
    query_nope,
    query_rope,
    latent,
    key_rope,
    latent_gain,
    key_up,
    value_up,
    out_proj,
    residual,
    ffn_gain,
    expert_ids,
    route_weights,
    expert_gate,
    expert_up,
    expert_down,
    shared_gate,
    shared_up,
    shared_down,
):
    row_count = latent.shape[0]
    first_row = lax.axis_index("sp") * row_count
    last_row = first_row + row_count - 1
    positions = first_row + jnp.arange(row_count, dtype=jnp.int32)
    local_heads = query_nope.shape[1] // NOPE
    head_start = lax.axis_index("tp") * local_heads
    key_local = lax.dynamic_slice_in_dim(key_up, head_start * NOPE, local_heads * NOPE, 1)
    value_local = lax.dynamic_slice_in_dim(value_up, head_start * VDIM, local_heads * VDIM, 1)
    normed_latent = scale_rows(latent, latent_gain)
    rot_key = rotate(key_rope[:, None, :], positions)[:, 0, :]
    queries_nope = query_nope.reshape(row_count, local_heads, NOPE)
    rot_query = rotate(query_rope.reshape(row_count, local_heads, ROPE), positions)
    score_scale = 1.0 / math.sqrt(NOPE + ROPE)

    def expand(block_latent):
        keys_flat = jnp.dot(block_latent, key_local, preferred_element_type=jnp.float32).astype(
            jnp.bfloat16
        )
        values_flat = jnp.dot(block_latent, value_local, preferred_element_type=jnp.float32).astype(
            jnp.bfloat16
        )
        return (keys_flat, values_flat)

    def attend(state_now, keys_flat, values_flat, keys_rope, key_start):
        running, weight_sum, weighted = state_now
        key_count = keys_flat.shape[0]
        key_heads = keys_flat.reshape(key_count, local_heads, NOPE)
        value_heads = values_flat.reshape(key_count, local_heads, VDIM)
        scores = jnp.einsum(
            "qhd,khd->hqk", queries_nope, key_heads, preferred_element_type=jnp.float32
        )
        scores = (
            scores
            + jnp.einsum("qhd,kd->hqk", rot_query, keys_rope, preferred_element_type=jnp.float32)
        ) * score_scale
        key_pos = key_start + jnp.arange(key_count, dtype=jnp.int32)
        allowed = (key_pos[None, :] <= positions[:, None])[None]
        scores = jnp.where(allowed, scores, -1e30)
        newest = jnp.maximum(running, jnp.max(scores, axis=-1))
        weights = jnp.where(allowed, jnp.exp(scores - newest[..., None]), 0.0)
        shrink = jnp.exp(running - newest)
        weight_sum = weight_sum * shrink + jnp.sum(weights, axis=-1)
        mixed = jnp.einsum(
            "hqk,khd->qhd",
            weights.astype(jnp.bfloat16),
            value_heads,
            preferred_element_type=jnp.float32,
        )
        weighted = weighted * shrink.T[:, :, None] + mixed
        return (newest, weight_sum, weighted)

    initial = (
        jnp.full((local_heads, row_count), -jnp.inf, jnp.float32),
        jnp.zeros((local_heads, row_count), jnp.float32),
        jnp.zeros((row_count, local_heads, VDIM), jnp.float32),
    )
    pieces = (
        lax.all_gather(normed_latent, "sp", axis=0, tiled=True),
        lax.all_gather(rot_key, "sp", axis=0, tiled=True),
    )
    piece_len = pieces[0].shape[0]
    span_len = math.gcd(piece_len, 1024)

    def advance(step_num, state_in):
        offset = step_num * span_len
        sliced = tuple((lax.dynamic_slice_in_dim(member, offset, span_len, 0) for member in pieces))

        def compute(state_cur):
            keys_flat, values_flat = expand(sliced[0])
            return attend(state_cur, keys_flat, values_flat, sliced[-1], offset)

        def unchanged(state_cur):
            return state_cur

        return lax.cond(offset <= last_row, compute, unchanged, state_in)

    folded = lax.fori_loop(0, piece_len // span_len, advance, initial)
    heads_out = (
        (folded[2] / folded[1].T[:, :, None])
        .astype(jnp.bfloat16)
        .reshape(row_count, local_heads * VDIM)
    )
    tokens = residual.shape[0]
    attn_sum = lax.psum_scatter(
        jnp.dot(heads_out, out_proj, preferred_element_type=jnp.float32).astype(jnp.bfloat16),
        "tp",
        scatter_dimension=0,
        tiled=True,
    ).astype(jnp.float32)
    hidden_one = (residual.astype(jnp.float32) + attn_sum).astype(jnp.bfloat16)
    normed = scale_rows(hidden_one, ffn_gain)
    slot_count = expert_ids.shape[1]
    model_width = residual.shape[1]
    local_experts = expert_gate.shape[0]
    experts = local_experts * lax.axis_size("sp")
    capacity = max(2, 2 * tokens * slot_count // experts)
    flat_ids = expert_ids.reshape(-1)
    onehot = (flat_ids[:, None] == jnp.arange(experts, dtype=jnp.int32)[None, :]).astype(jnp.int32)
    slot_rank = jnp.sum(jnp.cumsum(onehot, axis=0) * onehot, axis=1) - 1
    target = flat_ids * capacity + slot_rank
    slot_token = (
        jnp.full((experts * capacity,), tokens, jnp.int32)
        .at[target]
        .set(jnp.arange(tokens * slot_count, dtype=jnp.int32) // slot_count)
    )
    padded = jnp.concatenate([normed, jnp.zeros((1, model_width), jnp.bfloat16)], axis=0)
    outgoing = padded[slot_token].reshape(experts, capacity, model_width)
    arrived = lax.all_to_all(outgoing, "sp", split_axis=0, concat_axis=0, tiled=True)
    item_count = arrived.shape[1]
    grouped = arrived.reshape(-1, local_experts, item_count, model_width)
    gate_part = jnp.einsum(
        "seid,edf->seif", grouped, expert_gate, preferred_element_type=jnp.float32
    )
    upper_part = jnp.einsum(
        "seid,edf->seif", grouped, expert_up, preferred_element_type=jnp.float32
    )
    expert_hidden = (jax.nn.silu(gate_part) * upper_part).astype(jnp.bfloat16)
    expert_rows = jnp.einsum(
        "seif,efd->seid", expert_hidden, expert_down, preferred_element_type=jnp.float32
    ).astype(jnp.bfloat16)
    answered = expert_rows.reshape(-1, item_count, model_width)
    returned = lax.all_to_all(answered, "sp", split_axis=0, concat_axis=0, tiled=True)
    picked = returned.reshape(experts * capacity, model_width)[target]
    routed = jnp.sum(
        (picked.astype(jnp.float32) * route_weights.reshape(-1)[:, None]).reshape(
            tokens, slot_count, model_width
        ),
        axis=1,
    ).astype(jnp.bfloat16)
    shared_gate_part = jnp.dot(normed, shared_gate, preferred_element_type=jnp.float32)
    shared_upper = jnp.dot(normed, shared_up, preferred_element_type=jnp.float32)
    shared_hidden = (jax.nn.silu(shared_gate_part) * shared_upper).astype(jnp.bfloat16)
    shared_rows = jnp.dot(shared_hidden, shared_down, preferred_element_type=jnp.float32).astype(
        jnp.bfloat16
    )
    return (
        hidden_one.astype(jnp.float32)
        + routed.astype(jnp.float32)
        + shared_rows.astype(jnp.float32)
    ).astype(jnp.bfloat16)


MESH = pl.DeviceIdType.MESH
F32 = jnp.float32
BF16 = jnp.bfloat16
LANES = 128


def arrived(ref, sem):
    pltpu.make_async_copy(ref, ref, sem).wait()


def greet(z, depth, me, tp_peers):
    barrier = pltpu.get_barrier_semaphore()

    @pl.when(z + 1 < depth)
    def _():
        pl.semaphore_signal(barrier, inc=1, device_id={"sp": me + 2}, device_id_type=MESH)

    @pl.when(z > 0)
    def _():
        pl.semaphore_signal(barrier, inc=1, device_id={"sp": me - 2}, device_id_type=MESH)

    pair = z * 4 + 1 - me
    pl.semaphore_signal(barrier, inc=1, device_id={"sp": pair}, device_id_type=MESH)
    for peer in tp_peers:
        pl.semaphore_signal(barrier, inc=1, device_id={"tp": peer}, device_id_type=MESH)
    line_peers = (z + 1 < depth).astype(jnp.int32) + (z > 0).astype(jnp.int32)
    pl.semaphore_wait(barrier, 1 + len(tp_peers) + line_peers)


class Gather:
    def __init__(self, view, up, down, side, got, z, x, depth, relay=None):
        self.view, self.up, self.down, self.side, self.got = view, up, down, side, got
        self.z, self.x, self.depth, self.relay = z, x, depth, relay
        self.me = z * 2 + x

    def copy(self, block, sem, to):
        return pltpu.make_async_remote_copy(
            src_ref=self.view(block), dst_ref=self.view(block), send_sem=sem,
            recv_sem=self.got.at[block], device_id={"sp": to}, device_id_type=MESH)

    def send_up(self, zz):
        return self.copy(zz * 2 + self.x, self.up.at[zz], self.me + 2)

    def send_down(self, zz):
        return self.copy(zz * 2 + self.x, self.down.at[zz], self.me - 2)

    def send_side(self, zz):
        return self.copy(zz * 2 + self.x, self.side.at[zz], self.z * 2 + 1 - self.x)

    def start(self):
        z = self.z

        @pl.when(z + 1 < self.depth)
        def _():
            self.send_up(z).start()

        @pl.when(z > 0)
        def _():
            self.send_down(z).start()

        self.send_side(z).start()

    def run(self):
        z, x, depth = self.z, self.x, self.depth
        for j in range(1, depth):
            @pl.when(z - j >= 0)
            def _():
                zz = z - j
                arrived(self.view(zz * 2 + x), self.got.at[zz * 2 + x])

                @pl.when(z + 1 < depth)
                def _():
                    self.send_up(zz).start()

                self.send_side(zz).start()
                if self.relay is not None:
                    self.relay(zz * 2 + x)

            @pl.when(z + j < depth)
            def _():
                zz = z + j
                arrived(self.view(zz * 2 + x), self.got.at[zz * 2 + x])

                @pl.when(z > 0)
                def _():
                    self.send_down(zz).start()

                self.send_side(zz).start()
                if self.relay is not None:
                    self.relay(zz * 2 + x)

        def crossed(zz):
            block = zz * 2 + 1 - x
            arrived(self.view(block), self.got.at[block])
            if self.relay is not None:
                self.relay(block)

        crossed(z)
        for j in range(1, depth):
            @pl.when(z - j >= 0)
            def _():
                crossed(z - j)

            @pl.when(z + j < depth)
            def _():
                crossed(z + j)

    def finish(self):
        z, depth = self.z, self.depth
        for zz in range(depth):
            @pl.when((zz <= z) & (z + 1 < depth))
            def _():
                self.send_up(zz).wait_send()

            @pl.when((zz >= z) & (z > 0))
            def _():
                self.send_down(zz).wait_send()

            self.send_side(zz).wait_send()


def latent_kernel(depth, own_ref, out_ref, up, down, side, got, relay_out, relay_in):
    me = lax.axis_index("sp")
    t = lax.axis_index("tp")
    z, x = me // 2, me % 2
    half = t % 2
    sibling = t + 1 - 2 * half
    greet(z, depth, me, [sibling])
    out_ref[me] = own_ref[...]

    def relay_copy(block):
        return pltpu.make_async_remote_copy(
            src_ref=out_ref.at[block, half], dst_ref=out_ref.at[block, half],
            send_sem=relay_out.at[block], recv_sem=relay_in.at[block],
            device_id={"tp": sibling}, device_id_type=MESH)

    ring = Gather(lambda b: out_ref.at[b, half], up, down, side, got, z, x, depth,
                  relay=lambda b: relay_copy(b).start())
    ring.start()
    ring.run()
    for block in range(2 * depth):
        @pl.when(block != me)
        def _():
            arrived(out_ref.at[block, 1 - half], relay_in.at[block])
            relay_copy(block).wait_send()
    ring.finish()


def gather_latents(packed, sp):
    depth = sp // 2
    rows, width = packed.shape
    dma = pltpu.SemaphoreType.DMA
    out = pl.pallas_call(
        functools.partial(latent_kernel, depth),
        out_shape=jax.ShapeDtypeStruct((sp, 2, rows // 2, width), packed.dtype),
        in_specs=[pl.BlockSpec(memory_space=pltpu.VMEM)],
        out_specs=pl.BlockSpec(memory_space=pltpu.VMEM),
        scratch_shapes=[dma((depth,)), dma((depth,)), dma((depth,)), dma((sp,)), dma((sp,)), dma((sp,))],
        compiler_params=pltpu.CompilerParams(collective_id=0, has_side_effects=True),
        name="latent_gather",
    )(packed.reshape(2, rows // 2, width))
    return out.reshape(sp, rows, width)


def gated(rows, gate, up, down):
    gate_part = jnp.dot(rows, gate[...], preferred_element_type=F32)
    upper = jnp.dot(rows, up[...], preferred_element_type=F32)
    hidden = (gate_part / (1.0 + jnp.exp(-gate_part)) * upper).astype(BF16)
    return jnp.dot(hidden, down[...], preferred_element_type=F32).astype(BF16)


def tail_kernel(depth, chips, experts,
                heads_ref, proj_ref, resid_ref, gain_ref, route_ref,
                eg_hbm, eu_hbm, ed_hbm, sg_hbm, su_hbm, sd_hbm,
                out_ref,
                eg, eu, ed, sg, su, sd, load_sem,
                part, sib, ysend, yrecv, sib_s, sib_r, y_s, y_r,
                hid, shared, xbuf, up, down, side, got,
                contrib, xr, upr, dnr, rx_s, rx_r, rz_s, up_r, dn_r):
    me = lax.axis_index("sp")
    t = lax.axis_index("tp")
    z, x = me // 2, me % 2
    y, c = t // 2, t % 2
    tokens, width = resid_ref.shape
    loads = [pltpu.make_async_copy(src, dst, load_sem.at[i]) for i, (src, dst) in enumerate(
        ((sg_hbm, sg), (su_hbm, su), (sd_hbm, sd), (eg_hbm.at[0], eg), (eu_hbm.at[0], eu), (ed_hbm.at[0], ed)))]
    for load in loads:
        load.start()
    sibling = t + 1 - 2 * c
    peers = [lax.rem(t + 2 * d, 2 * chips) for d in range(1, chips)]
    greet(z, depth, me, [sibling] + peers)

    def project(block):
        rows = heads_ref[pl.ds(pl.multiple_of(block * tokens, tokens), tokens), :]
        return jnp.dot(rows, proj_ref[...], preferred_element_type=F32).astype(BF16)

    def to_sibling(yy):
        return pltpu.make_async_remote_copy(
            src_ref=part.at[yy], dst_ref=sib.at[yy], send_sem=sib_s.at[yy], recv_sem=sib_r.at[yy],
            device_id={"tp": sibling}, device_id_type=MESH)

    def to_chip(d):
        return pltpu.make_async_remote_copy(
            src_ref=ysend.at[d - 1], dst_ref=yrecv.at[d - 1], send_sem=y_s.at[d - 1], recv_sem=y_r.at[d - 1],
            device_id={"tp": peers[d - 1]}, device_id_type=MESH)

    ahead = [lax.rem(y + d, chips) for d in range(1, chips)] + [y]
    for yy in ahead:
        part[yy] = project(yy * 2 + 1 - c)
        to_sibling(yy).start()
    for d in range(1, chips):
        yy = ahead[d - 1]
        mine = project(yy * 2 + c).astype(F32)
        arrived(sib.at[yy], sib_r.at[yy])
        ysend[d - 1] = (mine + sib[yy].astype(F32)).astype(BF16)
        to_chip(d).start()
    total = project(y * 2 + c).astype(F32)
    arrived(sib.at[y], sib_r.at[y])
    total = total + sib[y].astype(F32)
    for d in range(1, chips):
        arrived(yrecv.at[d - 1], y_r.at[d - 1])
        total = total + yrecv[d - 1].astype(F32)
    hidden_one = (resid_ref[...].astype(F32) + total).astype(BF16)
    hid[...] = hidden_one
    wide = hidden_one.astype(F32)
    factor = lax.rsqrt(jnp.mean(wide * wide, axis=-1, keepdims=True) + norm_eps)
    xbuf[me, :, :width] = (wide * factor * gain_ref[...].astype(F32)).astype(BF16)
    xbuf[me, :, width:] = route_ref[...]

    ring = Gather(lambda b: xbuf.at[b], up, down, side, got, z, x, depth)
    ring.start()
    for load in loads[:3]:
        load.wait()
    shared[...] = gated(xbuf[me, :, :width], sg, su, sd)
    ring.run()
    for load in loads[3:]:
        load.wait()

    def cross(zz):
        return pltpu.make_async_remote_copy(
            src_ref=contrib.at[zz, 1 - x], dst_ref=xr.at[zz], send_sem=rx_s.at[zz], recv_sem=rx_r.at[zz],
            device_id={"sp": z * 2 + 1 - x}, device_id_type=MESH)

    high = (z >= depth // 2).astype(jnp.int32)

    def expert_step(j, carry):
        pick = high * j + (1 - high) * (depth - 2 - j)
        pick = pick + (pick >= z).astype(jnp.int32)
        last = (j == depth - 1).astype(jnp.int32)
        zz = last * z + (1 - last) * pick
        pair = xbuf[pl.ds(zz * 2, 2)].reshape(2 * tokens, width + LANES)
        routes = pair[:, width:].astype(F32)
        lane = lax.broadcasted_iota(jnp.int32, routes.shape, 1)
        weight = jnp.sum(jnp.where((lane == me) | (lane == me + experts), routes, 0.0), axis=1, keepdims=True)
        rows = gated(pair[:, :width], eg, eu, ed).astype(F32) * weight
        contrib[zz] = rows.astype(BF16).reshape(2, tokens, width)
        cross(zz).start()
        return carry

    lax.fori_loop(0, depth, expert_step, 0)

    def pass_up(dst):
        return pltpu.make_async_remote_copy(
            src_ref=contrib.at[dst, x], dst_ref=upr.at[dst], send_sem=rz_s.at[dst], recv_sem=up_r.at[dst],
            device_id={"sp": me + 2}, device_id_type=MESH)

    def pass_down(dst):
        return pltpu.make_async_remote_copy(
            src_ref=contrib.at[dst, x], dst_ref=dnr.at[dst], send_sem=rz_s.at[dst], recv_sem=dn_r.at[dst],
            device_id={"sp": me - 2}, device_id_type=MESH)

    def local_sum(dst):
        arrived(xr.at[dst], rx_r.at[dst])
        return contrib[dst, x].astype(F32) + xr[dst].astype(F32)

    for k in range(depth - 1):
        @pl.when(depth - 1 - k > z)
        def _():
            dst = depth - 1 - k

            @pl.when(z > 0)
            def _():
                arrived(upr.at[dst], up_r.at[dst])
                contrib[dst, x] = (local_sum(dst) + upr[dst].astype(F32)).astype(BF16)

            @pl.when(z == 0)
            def _():
                contrib[dst, x] = local_sum(dst).astype(BF16)

            pass_up(dst).start()

        @pl.when(k < z)
        def _():
            dst = k

            @pl.when(z + 1 < depth)
            def _():
                arrived(dnr.at[dst], dn_r.at[dst])
                contrib[dst, x] = (local_sum(dst) + dnr[dst].astype(F32)).astype(BF16)

            @pl.when(z + 1 == depth)
            def _():
                contrib[dst, x] = local_sum(dst).astype(BF16)

            pass_down(dst).start()

    @pl.when(z == 0)
    def _():
        upr[z] = jnp.zeros(upr.shape[1:], BF16)

    @pl.when(z > 0)
    def _():
        arrived(upr.at[z], up_r.at[z])

    @pl.when(z + 1 == depth)
    def _():
        dnr[z] = jnp.zeros(dnr.shape[1:], BF16)

    @pl.when(z + 1 < depth)
    def _():
        arrived(dnr.at[z], dn_r.at[z])

    routed = (local_sum(z) + upr[z].astype(F32) + dnr[z].astype(F32)).astype(BF16)
    out_ref[...] = (hid[...].astype(F32) + routed.astype(F32) + shared[...].astype(F32)).astype(BF16)

    for yy in range(chips):
        to_sibling(yy).wait_send()
    for d in range(1, chips):
        to_chip(d).wait_send()
    ring.finish()
    for zz in range(depth):
        cross(zz).wait_send()

        @pl.when(zz != z)
        def _():
            pltpu.make_async_copy(contrib.at[zz, x], contrib.at[zz, x], rz_s.at[zz]).wait()


def finish_layer(sp, tp, heads_out, out_proj, residual, ffn_gain, routes, eg, eu, ed, sg, su, sd):
    depth, chips = sp // 2, tp // 2
    tokens, width = residual.shape
    ff = sg.shape[1]
    dma = pltpu.SemaphoreType.DMA
    vmem = pl.BlockSpec(memory_space=pltpu.VMEM)
    hbm = pl.BlockSpec(memory_space=pl.ANY)
    block = (tokens, width)
    experts = sp

    def buf(*shape):
        return pltpu.VMEM(shape, BF16)

    scratch = [
        buf(width, ff), buf(width, ff), buf(ff, width), buf(width, ff), buf(width, ff), buf(ff, width), dma((6,)),
        buf(chips, *block), buf(chips, *block), buf(chips - 1, *block), buf(chips - 1, *block),
        dma((chips,)), dma((chips,)), dma((chips - 1,)), dma((chips - 1,)),
        buf(*block), buf(*block), buf(sp, tokens, width + LANES),
        dma((depth,)), dma((depth,)), dma((depth,)), dma((sp,)),
        buf(depth, 2, *block), buf(depth, *block), buf(depth, *block), buf(depth, *block),
        dma((depth,)), dma((depth,)), dma((depth,)), dma((depth,)), dma((depth,)),
    ]
    return pl.pallas_call(
        functools.partial(tail_kernel, depth, chips, experts),
        out_shape=jax.ShapeDtypeStruct(block, BF16),
        in_specs=[vmem] * 5 + [hbm] * 6,
        out_specs=vmem,
        scratch_shapes=scratch,
        compiler_params=pltpu.CompilerParams(
            collective_id=1, has_side_effects=True, vmem_limit_bytes=48 * 1024 * 1024),
        name="layer_tail",
    )(heads_out, out_proj, residual, ffn_gain.reshape(1, -1), routes, eg, eu, ed, sg, su, sd)


def attention(row_count, local_heads, queries_nope, rot_query, key_local, value_local, positions, last_row, pieces):
    score_scale = 1.0 / math.sqrt(NOPE + ROPE)

    def expand(block_latent):
        keys_flat = jnp.dot(block_latent, key_local, preferred_element_type=jnp.float32).astype(BF16)
        values_flat = jnp.dot(block_latent, value_local, preferred_element_type=jnp.float32).astype(BF16)
        return (keys_flat, values_flat)

    def attend(state_now, keys_flat, values_flat, keys_rope, key_start):
        running, weight_sum, weighted = state_now
        key_count = keys_flat.shape[0]
        key_heads = keys_flat.reshape(key_count, local_heads, NOPE)
        value_heads = values_flat.reshape(key_count, local_heads, VDIM)
        scores = jnp.einsum("qhd,khd->hqk", queries_nope, key_heads, preferred_element_type=jnp.float32)
        scores = (
            scores + jnp.einsum("qhd,kd->hqk", rot_query, keys_rope, preferred_element_type=jnp.float32)
        ) * score_scale
        key_pos = key_start + jnp.arange(key_count, dtype=jnp.int32)
        allowed = (key_pos[None, :] <= positions[:, None])[None]
        scores = jnp.where(allowed, scores, -1e30)
        newest = jnp.maximum(running, jnp.max(scores, axis=-1))
        weights = jnp.where(allowed, jnp.exp(scores - newest[..., None]), 0.0)
        shrink = jnp.exp(running - newest)
        weight_sum = weight_sum * shrink + jnp.sum(weights, axis=-1)
        mixed = jnp.einsum("hqk,khd->qhd", weights.astype(BF16), value_heads, preferred_element_type=jnp.float32)
        weighted = weighted * shrink.T[:, :, None] + mixed
        return (newest, weight_sum, weighted)

    initial = (
        jnp.full((local_heads, row_count), -jnp.inf, jnp.float32),
        jnp.zeros((local_heads, row_count), jnp.float32),
        jnp.zeros((row_count, local_heads, VDIM), jnp.float32),
    )
    piece_len = pieces[0].shape[0]
    span_len = math.gcd(piece_len, 1024)

    def advance(step_num, state_in):
        offset = step_num * span_len
        sliced = tuple((lax.dynamic_slice_in_dim(member, offset, span_len, 0) for member in pieces))

        def compute(state_cur):
            keys_flat, values_flat = expand(sliced[0])
            return attend(state_cur, keys_flat, values_flat, sliced[-1], offset)

        return lax.cond(offset <= last_row, compute, lambda state_cur: state_cur, state_in)

    folded = lax.fori_loop(0, piece_len // span_len, advance, initial)
    return (folded[2] / folded[1].T[:, :, None]).astype(BF16).reshape(row_count, local_heads * VDIM)


def line_body(query_nope, query_rope, latent, key_rope, latent_gain, key_up, value_up, out_proj, residual, ffn_gain,
              expert_ids, route_weights, expert_gate, expert_up, expert_down, shared_gate, shared_up, shared_down):
    sp, tp = lax.axis_size("sp"), lax.axis_size("tp")
    row_count, rank = latent.shape
    first_row = lax.axis_index("sp") * row_count
    last_row = first_row + row_count - 1
    positions = first_row + jnp.arange(row_count, dtype=jnp.int32)
    local_heads = query_nope.shape[1] // NOPE
    head_start = lax.axis_index("tp") * local_heads
    normed_latent = scale_rows(latent, latent_gain)
    rot_key = rotate(key_rope[:, None, :], positions)[:, 0, :]
    rope_rows = row_count * ROPE // rank
    packed = jnp.concatenate([normed_latent, rot_key.reshape(rope_rows, rank)], axis=0)
    gathered = gather_latents(packed, sp)
    pieces = (
        gathered[:, :row_count].reshape(sp * row_count, rank),
        gathered[:, row_count:].reshape(sp * row_count, ROPE),
    )
    key_local = lax.dynamic_slice_in_dim(key_up, head_start * NOPE, local_heads * NOPE, 1)
    value_local = lax.dynamic_slice_in_dim(value_up, head_start * VDIM, local_heads * VDIM, 1)
    queries_nope = query_nope.reshape(row_count, local_heads, NOPE)
    rot_query = rotate(query_rope.reshape(row_count, local_heads, ROPE), positions)
    heads_out = attention(
        row_count, local_heads, queries_nope, rot_query, key_local, value_local, positions, last_row, pieces)
    chosen = expert_ids[:, :, None] == jnp.arange(sp, dtype=jnp.int32)
    dense = jnp.sum(jnp.where(chosen, route_weights[:, :, None], 0.0), axis=1)
    coarse = lax.reduce_precision(dense, 8, 7)
    fine = dense - coarse
    routes = jnp.pad(jnp.concatenate([coarse, fine], axis=1), ((0, 0), (0, LANES - 2 * sp))).astype(BF16)
    return finish_layer(sp, tp, heads_out, out_proj, residual, ffn_gain, routes,
                        expert_gate, expert_up, expert_down, shared_gate, shared_up, shared_down)


def body(*args):
    latent, residual, expert_ids, expert_gate = args[2], args[8], args[10], args[12]
    sp, tp = lax.axis_size("sp"), lax.axis_size("tp")
    tokens, slots = residual.shape[0], expert_ids.shape[1]
    experts = expert_gate.shape[0] * sp
    capacity = 2 * tokens * slots // experts
    dense = capacity >= tokens and expert_gate.shape[0] == 1
    if dense and sp % 2 == 0 and tp % 2 == 0 and tp > 2 and 2 * sp <= LANES:
        return line_body(*args)
    return start_body(*args)


def solution(mesh):
    in_specs = (
        P("sp", "tp"),
        P("sp", "tp"),
        P("sp", None),
        P("sp", None),
        P(),
        P(),
        P(),
        P("tp", None),
        P(("sp", "tp"), None),
        P(),
        P(("sp", "tp"), None),
        P(("sp", "tp"), None),
        P("sp", None, None),
        P("sp", None, None),
        P("sp", None, None),
        P(),
        P(),
        P(),
    )
    out_specs = P(("sp", "tp"), None)
    return jax.shard_map(body, mesh=mesh, in_specs=in_specs, out_specs=out_specs, check_vma=False)
```

```python
import functools
import math

import jax
import jax.numpy as jnp
import numpy as np
from jax import lax
from jax.experimental import pallas as pl
from jax.experimental.pallas import tpu as pltpu
from jax.sharding import PartitionSpec as P

NOPE = 128
ROPE = 64
VDIM = 128


rope_base = 10000.0
norm_eps = 1e-06


def scale_rows(values, gain_vec):
    as_float = values.astype(jnp.float32)
    factor = lax.rsqrt(jnp.mean(as_float * as_float, axis=-1, keepdims=True) + norm_eps)
    return (as_float * factor * gain_vec.astype(jnp.float32)).astype(jnp.bfloat16)


def rotate(values, positions):
    half_dim = values.shape[-1] // 2
    frequency = rope_base ** (-jnp.arange(half_dim, dtype=jnp.float32) / half_dim)
    angles = positions.astype(jnp.float32)[:, None, None] * frequency
    cosine = jnp.cos(angles)
    sine_part = jnp.sin(angles)
    as_float = values.astype(jnp.float32)
    first_half = as_float[..., :half_dim]
    second_half = as_float[..., half_dim:]
    return jnp.concatenate(
        [
            first_half * cosine - second_half * sine_part,
            first_half * sine_part + second_half * cosine,
        ],
        axis=-1,
    ).astype(jnp.bfloat16)


def start_body(
    query_nope,
    query_rope,
    latent,
    key_rope,
    latent_gain,
    key_up,
    value_up,
    out_proj,
    residual,
    ffn_gain,
    expert_ids,
    route_weights,
    expert_gate,
    expert_up,
    expert_down,
    shared_gate,
    shared_up,
    shared_down,
):
    row_count = latent.shape[0]
    first_row = lax.axis_index("sp") * row_count
    last_row = first_row + row_count - 1
    positions = first_row + jnp.arange(row_count, dtype=jnp.int32)
    local_heads = query_nope.shape[1] // NOPE
    head_start = lax.axis_index("tp") * local_heads
    key_local = lax.dynamic_slice_in_dim(key_up, head_start * NOPE, local_heads * NOPE, 1)
    value_local = lax.dynamic_slice_in_dim(value_up, head_start * VDIM, local_heads * VDIM, 1)
    normed_latent = scale_rows(latent, latent_gain)
    rot_key = rotate(key_rope[:, None, :], positions)[:, 0, :]
    queries_nope = query_nope.reshape(row_count, local_heads, NOPE)
    rot_query = rotate(query_rope.reshape(row_count, local_heads, ROPE), positions)
    score_scale = 1.0 / math.sqrt(NOPE + ROPE)

    def expand(block_latent):
        keys_flat = jnp.dot(block_latent, key_local, preferred_element_type=jnp.float32).astype(
            jnp.bfloat16
        )
        values_flat = jnp.dot(block_latent, value_local, preferred_element_type=jnp.float32).astype(
            jnp.bfloat16
        )
        return (keys_flat, values_flat)

    def attend(state_now, keys_flat, values_flat, keys_rope, key_start):
        running, weight_sum, weighted = state_now
        key_count = keys_flat.shape[0]
        key_heads = keys_flat.reshape(key_count, local_heads, NOPE)
        value_heads = values_flat.reshape(key_count, local_heads, VDIM)
        scores = jnp.einsum(
            "qhd,khd->hqk", queries_nope, key_heads, preferred_element_type=jnp.float32
        )
        scores = (
            scores
            + jnp.einsum("qhd,kd->hqk", rot_query, keys_rope, preferred_element_type=jnp.float32)
        ) * score_scale
        key_pos = key_start + jnp.arange(key_count, dtype=jnp.int32)
        allowed = (key_pos[None, :] <= positions[:, None])[None]
        scores = jnp.where(allowed, scores, -1e30)
        newest = jnp.maximum(running, jnp.max(scores, axis=-1))
        weights = jnp.where(allowed, jnp.exp(scores - newest[..., None]), 0.0)
        shrink = jnp.exp(running - newest)
        weight_sum = weight_sum * shrink + jnp.sum(weights, axis=-1)
        mixed = jnp.einsum(
            "hqk,khd->qhd",
            weights.astype(jnp.bfloat16),
            value_heads,
            preferred_element_type=jnp.float32,
        )
        weighted = weighted * shrink.T[:, :, None] + mixed
        return (newest, weight_sum, weighted)

    initial = (
        jnp.full((local_heads, row_count), -jnp.inf, jnp.float32),
        jnp.zeros((local_heads, row_count), jnp.float32),
        jnp.zeros((row_count, local_heads, VDIM), jnp.float32),
    )
    pieces = (
        lax.all_gather(normed_latent, "sp", axis=0, tiled=True),
        lax.all_gather(rot_key, "sp", axis=0, tiled=True),
    )
    piece_len = pieces[0].shape[0]
    span_len = math.gcd(piece_len, 1024)

    def advance(step_num, state_in):
        offset = step_num * span_len
        sliced = tuple((lax.dynamic_slice_in_dim(member, offset, span_len, 0) for member in pieces))

        def compute(state_cur):
            keys_flat, values_flat = expand(sliced[0])
            return attend(state_cur, keys_flat, values_flat, sliced[-1], offset)

        def unchanged(state_cur):
            return state_cur

        return lax.cond(offset <= last_row, compute, unchanged, state_in)

    folded = lax.fori_loop(0, piece_len // span_len, advance, initial)
    heads_out = (
        (folded[2] / folded[1].T[:, :, None])
        .astype(jnp.bfloat16)
        .reshape(row_count, local_heads * VDIM)
    )
    tokens = residual.shape[0]
    attn_sum = lax.psum_scatter(
        jnp.dot(heads_out, out_proj, preferred_element_type=jnp.float32).astype(jnp.bfloat16),
        "tp",
        scatter_dimension=0,
        tiled=True,
    ).astype(jnp.float32)
    hidden_one = (residual.astype(jnp.float32) + attn_sum).astype(jnp.bfloat16)
    normed = scale_rows(hidden_one, ffn_gain)
    slot_count = expert_ids.shape[1]
    model_width = residual.shape[1]
    local_experts = expert_gate.shape[0]
    experts = local_experts * lax.axis_size("sp")
    capacity = max(2, 2 * tokens * slot_count // experts)
    flat_ids = expert_ids.reshape(-1)
    onehot = (flat_ids[:, None] == jnp.arange(experts, dtype=jnp.int32)[None, :]).astype(jnp.int32)
    slot_rank = jnp.sum(jnp.cumsum(onehot, axis=0) * onehot, axis=1) - 1
    target = flat_ids * capacity + slot_rank
    slot_token = (
        jnp.full((experts * capacity,), tokens, jnp.int32)
        .at[target]
        .set(jnp.arange(tokens * slot_count, dtype=jnp.int32) // slot_count)
    )
    padded = jnp.concatenate([normed, jnp.zeros((1, model_width), jnp.bfloat16)], axis=0)
    outgoing = padded[slot_token].reshape(experts, capacity, model_width)
    arrived = lax.all_to_all(outgoing, "sp", split_axis=0, concat_axis=0, tiled=True)
    item_count = arrived.shape[1]
    grouped = arrived.reshape(-1, local_experts, item_count, model_width)
    gate_part = jnp.einsum(
        "seid,edf->seif", grouped, expert_gate, preferred_element_type=jnp.float32
    )
    upper_part = jnp.einsum(
        "seid,edf->seif", grouped, expert_up, preferred_element_type=jnp.float32
    )
    expert_hidden = (jax.nn.silu(gate_part) * upper_part).astype(jnp.bfloat16)
    expert_rows = jnp.einsum(
        "seif,efd->seid", expert_hidden, expert_down, preferred_element_type=jnp.float32
    ).astype(jnp.bfloat16)
    answered = expert_rows.reshape(-1, item_count, model_width)
    returned = lax.all_to_all(answered, "sp", split_axis=0, concat_axis=0, tiled=True)
    picked = returned.reshape(experts * capacity, model_width)[target]
    routed = jnp.sum(
        (picked.astype(jnp.float32) * route_weights.reshape(-1)[:, None]).reshape(
            tokens, slot_count, model_width
        ),
        axis=1,
    ).astype(jnp.bfloat16)
    shared_gate_part = jnp.dot(normed, shared_gate, preferred_element_type=jnp.float32)
    shared_upper = jnp.dot(normed, shared_up, preferred_element_type=jnp.float32)
    shared_hidden = (jax.nn.silu(shared_gate_part) * shared_upper).astype(jnp.bfloat16)
    shared_rows = jnp.dot(shared_hidden, shared_down, preferred_element_type=jnp.float32).astype(
        jnp.bfloat16
    )
    return (
        hidden_one.astype(jnp.float32)
        + routed.astype(jnp.float32)
        + shared_rows.astype(jnp.float32)
    ).astype(jnp.bfloat16)


MESH = pl.DeviceIdType.MESH
F32 = jnp.float32
BF16 = jnp.bfloat16
LANES = 128


def arrived(ref, sem):
    pltpu.make_async_copy(ref, ref, sem).wait()


def greet(z, depth, me, tp_peers):
    barrier = pltpu.get_barrier_semaphore()

    @pl.when(z + 1 < depth)
    def _():
        pl.semaphore_signal(barrier, inc=1, device_id={"sp": me + 2}, device_id_type=MESH)

    @pl.when(z > 0)
    def _():
        pl.semaphore_signal(barrier, inc=1, device_id={"sp": me - 2}, device_id_type=MESH)

    pair = z * 4 + 1 - me
    pl.semaphore_signal(barrier, inc=1, device_id={"sp": pair}, device_id_type=MESH)
    for peer in tp_peers:
        pl.semaphore_signal(barrier, inc=1, device_id={"tp": peer}, device_id_type=MESH)
    line_peers = (z + 1 < depth).astype(jnp.int32) + (z > 0).astype(jnp.int32)
    pl.semaphore_wait(barrier, 1 + len(tp_peers) + line_peers)


class Gather:
    def __init__(self, view, chunks, up, down, side, got, z, x, depth, relay=None):
        self.view, self.up, self.down, self.side, self.got = view, up, down, side, got
        self.z, self.x, self.depth, self.chunks = z, x, depth, chunks
        self.relay = relay if relay is not None else (lambda block, ch: None)
        self.me = z * 2 + x

    def copy(self, block, ch, sem, to):
        return pltpu.make_async_remote_copy(
            src_ref=self.view(block, ch), dst_ref=self.view(block, ch), send_sem=sem,
            recv_sem=self.got.at[block, ch], device_id={"sp": to}, device_id_type=MESH)

    def send_up(self, zz, ch):
        return self.copy(zz * 2 + self.x, ch, self.up.at[zz, ch], self.me + 2)

    def send_down(self, zz, ch):
        return self.copy(zz * 2 + self.x, ch, self.down.at[zz, ch], self.me - 2)

    def send_side(self, zz, ch):
        return self.copy(zz * 2 + self.x, ch, self.side.at[zz, ch], self.z * 2 + 1 - self.x)

    def take(self, block, ch):
        arrived(self.view(block, ch), self.got.at[block, ch])

    def start(self):
        z = self.z
        for ch in range(self.chunks):
            @pl.when(z + 1 < self.depth)
            def _():
                self.send_up(z, ch).start()

            @pl.when(z > 0)
            def _():
                self.send_down(z, ch).start()

            self.send_side(z, ch).start()

    def run(self):
        z, x, depth = self.z, self.x, self.depth
        for j in range(1, depth):
            for ch in range(self.chunks):
                @pl.when(z - j >= 0)
                def _():
                    zz = z - j
                    self.take(zz * 2 + x, ch)

                    @pl.when(z + 1 < depth)
                    def _():
                        self.send_up(zz, ch).start()

                    self.send_side(zz, ch).start()
                    self.relay(zz * 2 + x, ch)

                @pl.when(z + j < depth)
                def _():
                    zz = z + j
                    self.take(zz * 2 + x, ch)

                    @pl.when(z > 0)
                    def _():
                        self.send_down(zz, ch).start()

                    self.send_side(zz, ch).start()
                    self.relay(zz * 2 + x, ch)

        def crossed(zz):
            block = zz * 2 + 1 - x
            for ch in range(self.chunks):
                self.take(block, ch)
                self.relay(block, ch)

        crossed(z)
        for j in range(1, depth):
            @pl.when(z - j >= 0)
            def _():
                crossed(z - j)

            @pl.when(z + j < depth)
            def _():
                crossed(z + j)

    def finish(self):
        z, depth = self.z, self.depth
        for zz in range(depth):
            for ch in range(self.chunks):
                @pl.when((zz <= z) & (z + 1 < depth))
                def _():
                    self.send_up(zz, ch).wait_send()

                @pl.when((zz >= z) & (z > 0))
                def _():
                    self.send_down(zz, ch).wait_send()

                self.send_side(zz, ch).wait_send()


def gated(rows, gate, up, down):
    gate_part = jnp.dot(rows, gate[...], preferred_element_type=F32)
    upper = jnp.dot(rows, up[...], preferred_element_type=F32)
    hidden = (gate_part / (1.0 + jnp.exp(-gate_part)) * upper).astype(BF16)
    return jnp.dot(hidden, down[...], preferred_element_type=F32).astype(BF16)


CHUNKS = 2


def rotated(values, cosine, sine):
    lane = lax.broadcasted_iota(jnp.int32, values.shape, 1)
    half = ROPE // 2
    swapped = jnp.where(lane % ROPE < half, pltpu.roll(values, LANES - half, 1), pltpu.roll(values, half, 1))
    return values * cosine + swapped * sine


def layer_kernel(depth, chips, experts,
                 nope_ref, rope_ref, latent_ref, key_ref, latent_gain_ref, resid_ref, gain_ref, ids_ref, route_ref,
                 table_hbm, kup_hbm, vup_hbm, proj_hbm, eg_hbm, eu_hbm, ed_hbm, sg_hbm, su_hbm, sd_hbm,
                 out_ref,
                 table, kup, vup, proj_ref, eg, eu, ed, sg, su, sd, load_sem,
                 lat, query, heads_ref, mixed, l_up, l_down, l_side, l_got, relay_out, relay_in,
                 part, sib, ysend, yrecv, sib_s, sib_r, y_s, y_r,
                 hid, shared, xbuf, up, down, side, got,
                 contrib, xr, upr, dnr, rx_s, rx_r, rz_s, up_r, dn_r):
    me = lax.axis_index("sp")
    t = lax.axis_index("tp")
    z, x = me // 2, me % 2
    y, c = t // 2, t % 2
    tokens, width = resid_ref.shape
    rows, rank = latent_ref.shape
    head_cols = nope_ref.shape[1]
    local_heads = head_cols // NOPE
    columns = pl.ds(pl.multiple_of(t * head_cols, head_cols), head_cols)
    loads = [pltpu.make_async_copy(src, dst, load_sem.at[i]) for i, (src, dst) in enumerate(
        ((table_hbm.at[pl.ds(pl.multiple_of(me * rows, rows), rows)], table),
         (kup_hbm.at[:, columns], kup), (vup_hbm.at[:, columns], vup), (proj_hbm, proj_ref),
         (sg_hbm, sg), (su_hbm, su), (sd_hbm, sd), (eg_hbm.at[0], eg), (eu_hbm.at[0], eu), (ed_hbm.at[0], ed)))]
    for load in loads:
        load.start()
    sibling = t + 1 - 2 * c
    peers = [lax.rem(t + 2 * d, 2 * chips) for d in range(1, chips)]
    greet(z, depth, me, [sibling] + peers)

    wide = latent_ref[...].astype(F32)
    factor = lax.rsqrt(jnp.mean(wide * wide, axis=-1, keepdims=True) + norm_eps)
    lat[me, :, :rank] = (wide * factor * latent_gain_ref[...].astype(F32)).astype(BF16)
    loads[0].wait()
    cosine, sine = table[:, :ROPE], table[:, ROPE:]
    cosine = jnp.concatenate([cosine, cosine], axis=1)
    sine = jnp.concatenate([sine, sine], axis=1)
    key = key_ref[...].astype(F32)
    lat[me, :, rank:] = rotated(jnp.concatenate([key, key], axis=1), cosine, sine).astype(BF16)

    half_rows = rows // 2

    def half_view(block, half):
        return lat.at[block, pl.ds(pl.multiple_of(half * half_rows, half_rows), half_rows)]

    def relay_copy(block):
        return pltpu.make_async_remote_copy(
            src_ref=half_view(block, c), dst_ref=half_view(block, c),
            send_sem=relay_out.at[block], recv_sem=relay_in.at[block],
            device_id={"tp": sibling}, device_id_type=MESH)

    latents = Gather(lambda b, ch: half_view(b, c), 1, l_up, l_down, l_side, l_got, z, x, depth,
                     relay=lambda b, ch: relay_copy(b).start())
    latents.start()
    lane = lax.broadcasted_iota(jnp.int32, (rows, LANES), 1)
    turned = rotated(rope_ref[...].astype(F32), cosine, sine)
    for h in range(local_heads):
        query[h, :, :NOPE] = nope_ref[:, h * NOPE:(h + 1) * NOPE]
        query[h, :, NOPE:] = jnp.where(lane // ROPE == h, turned, 0.0).astype(BF16)
    lane = lax.broadcasted_iota(jnp.int32, (tokens, LANES), 1)
    dense = jnp.zeros((tokens, LANES), F32)
    for k in range(ids_ref.shape[1]):
        dense = dense + jnp.where(lane % experts == ids_ref[:, k:k + 1], route_ref[:, k:k + 1], 0.0)
    coarse = dense.astype(BF16).astype(F32)
    terms = jnp.where(lane < experts, coarse, jnp.where(lane < 2 * experts, dense - coarse, 0.0))
    xbuf[me, :, width:] = terms.astype(BF16)
    loads[1].wait()
    loads[2].wait()
    value_t = vup[...].astype(F32).T.astype(BF16)
    vup[...] = value_t
    latents.run()
    for block in range(2 * depth):
        @pl.when(block != me)
        def _():
            arrived(half_view(block, 1 - c), relay_in.at[block])

    span = 2 * rows
    score_scale = 1.0 / math.sqrt(NOPE + ROPE)
    mixed[...] = jnp.zeros(mixed.shape, F32)

    def attend(zz, state):
        pair = lat[pl.ds(zz * 2, 2)].reshape(span, rank + LANES)
        keys = jnp.dot(pair[:, :rank], kup[...], preferred_element_type=F32).astype(BF16)
        values_t = lax.dot_general(
            vup[...], pair[:, :rank], (((1,), (1,)), ((), ())), preferred_element_type=F32).astype(BF16)
        key_pos = zz * span + lax.broadcasted_iota(jnp.int32, (span, rows), 0)
        query_pos = me * rows + lax.broadcasted_iota(jnp.int32, (span, rows), 1)
        allowed = key_pos <= query_pos
        fresh = []
        for h in range(local_heads):
            top, weight_sum = state[h]
            full = jnp.concatenate([keys[:, h * NOPE:(h + 1) * NOPE], pair[:, rank:]], axis=1)
            scores = lax.dot_general(
                full, query[h], (((1,), (1,)), ((), ())), preferred_element_type=F32) * score_scale
            scores = jnp.where(allowed, scores, -1e30)
            newest = jnp.maximum(top, jnp.max(scores, axis=0, keepdims=True))
            weights = jnp.exp(scores - newest)
            shrink = jnp.exp(top - newest)
            weight_sum = weight_sum * shrink + jnp.sum(weights, axis=0, keepdims=True)
            mixed[h] = mixed[h] * shrink + jnp.dot(
                values_t[h * VDIM:(h + 1) * VDIM], weights.astype(BF16), preferred_element_type=F32)
            fresh.append((newest, weight_sum))
        return tuple(fresh)

    first = tuple((jnp.full((1, rows), -1e30, F32), jnp.zeros((1, rows), F32)) for _ in range(local_heads))
    folded = lax.fori_loop(0, z + 1, attend, first)
    for h in range(local_heads):
        heads_ref[:, h * VDIM:(h + 1) * VDIM] = (mixed[h] / folded[h][1]).T.astype(BF16)
    loads[3].wait()

    def project(block):
        mine = heads_ref[pl.ds(pl.multiple_of(block * tokens, tokens), tokens), :]
        return jnp.dot(mine, proj_ref[...], preferred_element_type=F32).astype(BF16)

    def to_sibling(yy):
        return pltpu.make_async_remote_copy(
            src_ref=part.at[yy], dst_ref=sib.at[yy], send_sem=sib_s.at[yy], recv_sem=sib_r.at[yy],
            device_id={"tp": sibling}, device_id_type=MESH)

    def to_chip(d):
        return pltpu.make_async_remote_copy(
            src_ref=ysend.at[d - 1], dst_ref=yrecv.at[d - 1], send_sem=y_s.at[d - 1], recv_sem=y_r.at[d - 1],
            device_id={"tp": peers[d - 1]}, device_id_type=MESH)

    ahead = [lax.rem(y + d, chips) for d in range(1, chips)] + [y]
    for yy in ahead:
        part[yy] = project(yy * 2 + 1 - c)
        to_sibling(yy).start()
    for d in range(1, chips):
        yy = ahead[d - 1]
        mine = project(yy * 2 + c).astype(F32)
        arrived(sib.at[yy], sib_r.at[yy])
        ysend[d - 1] = (mine + sib[yy].astype(F32)).astype(BF16)
        to_chip(d).start()
    total = project(y * 2 + c).astype(F32)
    arrived(sib.at[y], sib_r.at[y])
    total = total + sib[y].astype(F32)
    for d in range(1, chips):
        arrived(yrecv.at[d - 1], y_r.at[d - 1])
        total = total + yrecv[d - 1].astype(F32)
    hidden_one = (resid_ref[...].astype(F32) + total).astype(BF16)
    hid[...] = hidden_one
    wide = hidden_one.astype(F32)
    factor = lax.rsqrt(jnp.mean(wide * wide, axis=-1, keepdims=True) + norm_eps)
    xbuf[me, :, :width] = (wide * factor * gain_ref[...].astype(F32)).astype(BF16)

    piece = tokens // CHUNKS
    ring = Gather(lambda b, ch: xbuf.at[b, pl.ds(ch * piece, piece)], CHUNKS, up, down, side, got, z, x, depth)
    ring.start()
    for load in loads[4:7]:
        load.wait()
    shared[...] = gated(xbuf[me, :, :width], sg, su, sd)
    ring.run()
    for load in loads[7:]:
        load.wait()

    def cross(zz, ch):
        return pltpu.make_async_remote_copy(
            src_ref=contrib.at[zz, 1 - x, pl.ds(ch * piece, piece)], dst_ref=xr.at[zz, pl.ds(ch * piece, piece)],
            send_sem=rx_s.at[zz, ch], recv_sem=rx_r.at[zz, ch],
            device_id={"sp": z * 2 + 1 - x}, device_id_type=MESH)

    high = (z >= depth // 2).astype(jnp.int32)

    def expert_step(j, carry):
        pick = high * j + (1 - high) * (depth - 2 - j)
        pick = pick + (pick >= z).astype(jnp.int32)
        last = (j == depth - 1).astype(jnp.int32)
        zz = last * z + (1 - last) * pick
        pair = xbuf[pl.ds(zz * 2, 2)].reshape(2 * tokens, width + LANES)
        routes = pair[:, width:].astype(F32)
        lane = lax.broadcasted_iota(jnp.int32, routes.shape, 1)
        weight = jnp.sum(jnp.where((lane == me) | (lane == me + experts), routes, 0.0), axis=1, keepdims=True)
        answer = gated(pair[:, :width], eg, eu, ed).astype(F32) * weight
        contrib[zz] = answer.astype(BF16).reshape(2, tokens, width)
        for ch in range(CHUNKS):
            cross(zz, ch).start()
        return carry

    lax.fori_loop(0, depth, expert_step, 0)

    def pass_on(dst, ch, landing, recv, to):
        return pltpu.make_async_remote_copy(
            src_ref=contrib.at[dst, x, pl.ds(ch * piece, piece)], dst_ref=landing.at[dst, pl.ds(ch * piece, piece)],
            send_sem=rz_s.at[dst, ch], recv_sem=recv.at[dst, ch],
            device_id={"sp": to}, device_id_type=MESH)

    def local_sum(dst, ch):
        here = pl.ds(ch * piece, piece)
        arrived(xr.at[dst, here], rx_r.at[dst, ch])
        return contrib[dst, x, here].astype(F32) + xr[dst, here].astype(F32)

    def hop(dst, ch, landing, recv, at_end, to):
        here = pl.ds(ch * piece, piece)

        @pl.when(jnp.logical_not(at_end))
        def _():
            partial = local_sum(dst, ch)
            arrived(landing.at[dst, here], recv.at[dst, ch])
            contrib[dst, x, here] = (partial + landing[dst, here].astype(F32)).astype(BF16)

        @pl.when(at_end)
        def _():
            contrib[dst, x, here] = local_sum(dst, ch).astype(BF16)

        pass_on(dst, ch, landing, recv, to).start()

    for k in range(depth - 1):
        for ch in range(CHUNKS):
            @pl.when(depth - 1 - k > z)
            def _():
                hop(depth - 1 - k, ch, upr, up_r, z == 0, me + 2)

            @pl.when(k < z)
            def _():
                hop(k, ch, dnr, dn_r, z + 1 == depth, me - 2)

    @pl.when(z == 0)
    def _():
        upr[z] = jnp.zeros(upr.shape[1:], BF16)

    @pl.when(z + 1 == depth)
    def _():
        dnr[z] = jnp.zeros(dnr.shape[1:], BF16)

    for ch in range(CHUNKS):
        here = pl.ds(ch * piece, piece)

        @pl.when(z > 0)
        def _():
            arrived(upr.at[z, here], up_r.at[z, ch])

        @pl.when(z + 1 < depth)
        def _():
            arrived(dnr.at[z, here], dn_r.at[z, ch])

        routed = (local_sum(z, ch) + upr[z, here].astype(F32) + dnr[z, here].astype(F32)).astype(BF16)
        out_ref[here] = (hid[here].astype(F32) + routed.astype(F32) + shared[here].astype(F32)).astype(BF16)

    latents.finish()
    for block in range(2 * depth):
        @pl.when(block != me)
        def _():
            relay_copy(block).wait_send()
    for yy in range(chips):
        to_sibling(yy).wait_send()
    for d in range(1, chips):
        to_chip(d).wait_send()
    ring.finish()
    for zz in range(depth):
        for ch in range(CHUNKS):
            cross(zz, ch).wait_send()

            @pl.when(zz != z)
            def _():
                arrived(contrib.at[zz, x, pl.ds(ch * piece, piece)], rz_s.at[zz, ch])


def line_body(query_nope, query_rope, latent, key_rope, latent_gain, key_up, value_up, out_proj, residual, ffn_gain,
              expert_ids, route_weights, expert_gate, expert_up, expert_down, shared_gate, shared_up, shared_down):
    sp, tp = lax.axis_size("sp"), lax.axis_size("tp")
    depth, chips = sp // 2, tp // 2
    rows, rank = latent.shape
    tokens, width = residual.shape
    ff = shared_gate.shape[1]
    head_cols = query_nope.shape[1]
    half_dim = ROPE // 2
    frequency = np.float32(rope_base) ** (-np.arange(half_dim, dtype=np.float32) / np.float32(half_dim))
    angles = np.arange(sp * rows, dtype=np.float32)[:, None] * frequency[None, :]
    cosine, sine = np.cos(angles), np.sin(angles)
    table = jnp.asarray(np.concatenate([cosine, cosine, -sine, sine], axis=1), F32)
    dma = pltpu.SemaphoreType.DMA
    vmem = pl.BlockSpec(memory_space=pltpu.VMEM)
    hbm = pl.BlockSpec(memory_space=pl.ANY)
    block = (tokens, width)

    def buf(*shape):
        return pltpu.VMEM(shape, BF16)

    scratch = [
        pltpu.VMEM((rows, 2 * ROPE), F32), buf(rank, head_cols), buf(rank, head_cols), buf(head_cols, width),
        buf(width, ff), buf(width, ff), buf(ff, width), buf(width, ff), buf(width, ff), buf(ff, width), dma((10,)),
        buf(sp, rows, rank + LANES), buf(head_cols // NOPE, rows, NOPE + LANES), buf(rows, head_cols),
        pltpu.VMEM((head_cols // VDIM, VDIM, rows), F32),
        dma((depth, 1)), dma((depth, 1)), dma((depth, 1)), dma((sp, 1)), dma((sp,)), dma((sp,)),
        buf(chips, *block), buf(chips, *block), buf(chips - 1, *block), buf(chips - 1, *block),
        dma((chips,)), dma((chips,)), dma((chips - 1,)), dma((chips - 1,)),
        buf(*block), buf(*block), buf(sp, tokens, width + LANES),
        dma((depth, CHUNKS)), dma((depth, CHUNKS)), dma((depth, CHUNKS)), dma((sp, CHUNKS)),
        buf(depth, 2, *block), buf(depth, *block), buf(depth, *block), buf(depth, *block),
    ] + [dma((depth, CHUNKS))] * 5
    return pl.pallas_call(
        functools.partial(layer_kernel, depth, chips, sp),
        out_shape=jax.ShapeDtypeStruct(block, BF16),
        in_specs=[vmem] * 9 + [hbm] * 10,
        out_specs=vmem,
        scratch_shapes=scratch,
        compiler_params=pltpu.CompilerParams(
            collective_id=0, has_side_effects=True, vmem_limit_bytes=48 * 1024 * 1024),
        name="layer",
    )(query_nope, query_rope, latent, key_rope, latent_gain.reshape(1, -1), residual, ffn_gain.reshape(1, -1),
      expert_ids, route_weights, table, key_up, value_up, out_proj,
      expert_gate, expert_up, expert_down, shared_gate, shared_up, shared_down)


def body(*args):
    latent, residual, expert_ids, expert_gate = args[2], args[8], args[10], args[12]
    sp, tp = lax.axis_size("sp"), lax.axis_size("tp")
    tokens, slots = residual.shape[0], expert_ids.shape[1]
    experts = expert_gate.shape[0] * sp
    capacity = 2 * tokens * slots // experts
    dense = capacity >= tokens and expert_gate.shape[0] == 1 and args[0].shape[1] == 2 * NOPE == latent.shape[1]
    if dense and sp % 2 == 0 and tp % 2 == 0 and tp > 2 and 2 * sp <= LANES:
        return line_body(*args)
    return start_body(*args)


def solution(mesh):
    in_specs = (
        P("sp", "tp"),
        P("sp", "tp"),
        P("sp", None),
        P("sp", None),
        P(),
        P(),
        P(),
        P("tp", None),
        P(("sp", "tp"), None),
        P(),
        P(("sp", "tp"), None),
        P(("sp", "tp"), None),
        P("sp", None, None),
        P("sp", None, None),
        P("sp", None, None),
        P(),
        P(),
        P(),
    )
    out_specs = P(("sp", "tp"), None)
    return jax.shard_map(body, mesh=mesh, in_specs=in_specs, out_specs=out_specs, check_vma=False)
```

```python
import functools
import math

import jax
import jax.numpy as jnp
import numpy as np
from jax import lax
from jax.experimental import pallas as pl
from jax.experimental.pallas import tpu as pltpu
from jax.sharding import PartitionSpec as P

NOPE = 128
ROPE = 64
VDIM = 128


rope_base = 10000.0
norm_eps = 1e-06


def scale_rows(values, gain_vec):
    as_float = values.astype(jnp.float32)
    factor = lax.rsqrt(jnp.mean(as_float * as_float, axis=-1, keepdims=True) + norm_eps)
    return (as_float * factor * gain_vec.astype(jnp.float32)).astype(jnp.bfloat16)


def rotate(values, positions):
    half_dim = values.shape[-1] // 2
    frequency = rope_base ** (-jnp.arange(half_dim, dtype=jnp.float32) / half_dim)
    angles = positions.astype(jnp.float32)[:, None, None] * frequency
    cosine = jnp.cos(angles)
    sine_part = jnp.sin(angles)
    as_float = values.astype(jnp.float32)
    first_half = as_float[..., :half_dim]
    second_half = as_float[..., half_dim:]
    return jnp.concatenate(
        [
            first_half * cosine - second_half * sine_part,
            first_half * sine_part + second_half * cosine,
        ],
        axis=-1,
    ).astype(jnp.bfloat16)


def start_body(
    query_nope,
    query_rope,
    latent,
    key_rope,
    latent_gain,
    key_up,
    value_up,
    out_proj,
    residual,
    ffn_gain,
    expert_ids,
    route_weights,
    expert_gate,
    expert_up,
    expert_down,
    shared_gate,
    shared_up,
    shared_down,
):
    row_count = latent.shape[0]
    first_row = lax.axis_index("sp") * row_count
    last_row = first_row + row_count - 1
    positions = first_row + jnp.arange(row_count, dtype=jnp.int32)
    local_heads = query_nope.shape[1] // NOPE
    head_start = lax.axis_index("tp") * local_heads
    key_local = lax.dynamic_slice_in_dim(key_up, head_start * NOPE, local_heads * NOPE, 1)
    value_local = lax.dynamic_slice_in_dim(value_up, head_start * VDIM, local_heads * VDIM, 1)
    normed_latent = scale_rows(latent, latent_gain)
    rot_key = rotate(key_rope[:, None, :], positions)[:, 0, :]
    queries_nope = query_nope.reshape(row_count, local_heads, NOPE)
    rot_query = rotate(query_rope.reshape(row_count, local_heads, ROPE), positions)
    score_scale = 1.0 / math.sqrt(NOPE + ROPE)

    def expand(block_latent):
        keys_flat = jnp.dot(block_latent, key_local, preferred_element_type=jnp.float32).astype(
            jnp.bfloat16
        )
        values_flat = jnp.dot(block_latent, value_local, preferred_element_type=jnp.float32).astype(
            jnp.bfloat16
        )
        return (keys_flat, values_flat)

    def attend(state_now, keys_flat, values_flat, keys_rope, key_start):
        running, weight_sum, weighted = state_now
        key_count = keys_flat.shape[0]
        key_heads = keys_flat.reshape(key_count, local_heads, NOPE)
        value_heads = values_flat.reshape(key_count, local_heads, VDIM)
        scores = jnp.einsum(
            "qhd,khd->hqk", queries_nope, key_heads, preferred_element_type=jnp.float32
        )
        scores = (
            scores
            + jnp.einsum("qhd,kd->hqk", rot_query, keys_rope, preferred_element_type=jnp.float32)
        ) * score_scale
        key_pos = key_start + jnp.arange(key_count, dtype=jnp.int32)
        allowed = (key_pos[None, :] <= positions[:, None])[None]
        scores = jnp.where(allowed, scores, -1e30)
        newest = jnp.maximum(running, jnp.max(scores, axis=-1))
        weights = jnp.where(allowed, jnp.exp(scores - newest[..., None]), 0.0)
        shrink = jnp.exp(running - newest)
        weight_sum = weight_sum * shrink + jnp.sum(weights, axis=-1)
        mixed = jnp.einsum(
            "hqk,khd->qhd",
            weights.astype(jnp.bfloat16),
            value_heads,
            preferred_element_type=jnp.float32,
        )
        weighted = weighted * shrink.T[:, :, None] + mixed
        return (newest, weight_sum, weighted)

    initial = (
        jnp.full((local_heads, row_count), -jnp.inf, jnp.float32),
        jnp.zeros((local_heads, row_count), jnp.float32),
        jnp.zeros((row_count, local_heads, VDIM), jnp.float32),
    )
    pieces = (
        lax.all_gather(normed_latent, "sp", axis=0, tiled=True),
        lax.all_gather(rot_key, "sp", axis=0, tiled=True),
    )
    piece_len = pieces[0].shape[0]
    span_len = math.gcd(piece_len, 1024)

    def advance(step_num, state_in):
        offset = step_num * span_len
        sliced = tuple((lax.dynamic_slice_in_dim(member, offset, span_len, 0) for member in pieces))

        def compute(state_cur):
            keys_flat, values_flat = expand(sliced[0])
            return attend(state_cur, keys_flat, values_flat, sliced[-1], offset)

        def unchanged(state_cur):
            return state_cur

        return lax.cond(offset <= last_row, compute, unchanged, state_in)

    folded = lax.fori_loop(0, piece_len // span_len, advance, initial)
    heads_out = (
        (folded[2] / folded[1].T[:, :, None])
        .astype(jnp.bfloat16)
        .reshape(row_count, local_heads * VDIM)
    )
    tokens = residual.shape[0]
    attn_sum = lax.psum_scatter(
        jnp.dot(heads_out, out_proj, preferred_element_type=jnp.float32).astype(jnp.bfloat16),
        "tp",
        scatter_dimension=0,
        tiled=True,
    ).astype(jnp.float32)
    hidden_one = (residual.astype(jnp.float32) + attn_sum).astype(jnp.bfloat16)
    normed = scale_rows(hidden_one, ffn_gain)
    slot_count = expert_ids.shape[1]
    model_width = residual.shape[1]
    local_experts = expert_gate.shape[0]
    experts = local_experts * lax.axis_size("sp")
    capacity = max(2, 2 * tokens * slot_count // experts)
    flat_ids = expert_ids.reshape(-1)
    onehot = (flat_ids[:, None] == jnp.arange(experts, dtype=jnp.int32)[None, :]).astype(jnp.int32)
    slot_rank = jnp.sum(jnp.cumsum(onehot, axis=0) * onehot, axis=1) - 1
    target = flat_ids * capacity + slot_rank
    slot_token = (
        jnp.full((experts * capacity,), tokens, jnp.int32)
        .at[target]
        .set(jnp.arange(tokens * slot_count, dtype=jnp.int32) // slot_count)
    )
    padded = jnp.concatenate([normed, jnp.zeros((1, model_width), jnp.bfloat16)], axis=0)
    outgoing = padded[slot_token].reshape(experts, capacity, model_width)
    arrived = lax.all_to_all(outgoing, "sp", split_axis=0, concat_axis=0, tiled=True)
    item_count = arrived.shape[1]
    grouped = arrived.reshape(-1, local_experts, item_count, model_width)
    gate_part = jnp.einsum(
        "seid,edf->seif", grouped, expert_gate, preferred_element_type=jnp.float32
    )
    upper_part = jnp.einsum(
        "seid,edf->seif", grouped, expert_up, preferred_element_type=jnp.float32
    )
    expert_hidden = (jax.nn.silu(gate_part) * upper_part).astype(jnp.bfloat16)
    expert_rows = jnp.einsum(
        "seif,efd->seid", expert_hidden, expert_down, preferred_element_type=jnp.float32
    ).astype(jnp.bfloat16)
    answered = expert_rows.reshape(-1, item_count, model_width)
    returned = lax.all_to_all(answered, "sp", split_axis=0, concat_axis=0, tiled=True)
    picked = returned.reshape(experts * capacity, model_width)[target]
    routed = jnp.sum(
        (picked.astype(jnp.float32) * route_weights.reshape(-1)[:, None]).reshape(
            tokens, slot_count, model_width
        ),
        axis=1,
    ).astype(jnp.bfloat16)
    shared_gate_part = jnp.dot(normed, shared_gate, preferred_element_type=jnp.float32)
    shared_upper = jnp.dot(normed, shared_up, preferred_element_type=jnp.float32)
    shared_hidden = (jax.nn.silu(shared_gate_part) * shared_upper).astype(jnp.bfloat16)
    shared_rows = jnp.dot(shared_hidden, shared_down, preferred_element_type=jnp.float32).astype(
        jnp.bfloat16
    )
    return (
        hidden_one.astype(jnp.float32)
        + routed.astype(jnp.float32)
        + shared_rows.astype(jnp.float32)
    ).astype(jnp.bfloat16)


MESH = pl.DeviceIdType.MESH
F32 = jnp.float32
BF16 = jnp.bfloat16
LANES = 128


def arrived(ref, sem):
    pltpu.make_async_copy(ref, ref, sem).wait()


def greet(z, depth, me, tp_peers):
    barrier = pltpu.get_barrier_semaphore()

    @pl.when(z + 1 < depth)
    def _():
        pl.semaphore_signal(barrier, inc=1, device_id={"sp": me + 2}, device_id_type=MESH)

    @pl.when(z > 0)
    def _():
        pl.semaphore_signal(barrier, inc=1, device_id={"sp": me - 2}, device_id_type=MESH)

    pair = z * 4 + 1 - me
    pl.semaphore_signal(barrier, inc=1, device_id={"sp": pair}, device_id_type=MESH)
    for peer in tp_peers:
        pl.semaphore_signal(barrier, inc=1, device_id={"tp": peer}, device_id_type=MESH)
    line_peers = (z + 1 < depth).astype(jnp.int32) + (z > 0).astype(jnp.int32)
    pl.semaphore_wait(barrier, 1 + len(tp_peers) + line_peers)


class Gather:
    def __init__(self, view, chunks, up, down, side, got, z, x, depth, relay=None):
        self.view, self.up, self.down, self.side, self.got = view, up, down, side, got
        self.z, self.x, self.depth, self.chunks = z, x, depth, chunks
        self.relay = relay if relay is not None else (lambda block, ch: None)
        self.me = z * 2 + x

    def copy(self, block, ch, sem, to):
        return pltpu.make_async_remote_copy(
            src_ref=self.view(block, ch), dst_ref=self.view(block, ch), send_sem=sem,
            recv_sem=self.got.at[block, ch], device_id={"sp": to}, device_id_type=MESH)

    def send_up(self, zz, ch):
        return self.copy(zz * 2 + self.x, ch, self.up.at[zz, ch], self.me + 2)

    def send_down(self, zz, ch):
        return self.copy(zz * 2 + self.x, ch, self.down.at[zz, ch], self.me - 2)

    def send_side(self, zz, ch):
        return self.copy(zz * 2 + self.x, ch, self.side.at[zz, ch], self.z * 2 + 1 - self.x)

    def take(self, block, ch):
        arrived(self.view(block, ch), self.got.at[block, ch])

    def start(self, ch):
        z = self.z

        @pl.when(z + 1 < self.depth)
        def _():
            self.send_up(z, ch).start()

        @pl.when(z > 0)
        def _():
            self.send_down(z, ch).start()

        self.send_side(z, ch).start()

    def run(self, ready=None):
        z, x, depth = self.z, self.x, self.depth
        for j in range(1, depth):
            for ch in range(self.chunks):
                @pl.when(z - j >= 0)
                def _():
                    zz = z - j
                    self.take(zz * 2 + x, ch)

                    @pl.when(z + 1 < depth)
                    def _():
                        self.send_up(zz, ch).start()

                    self.send_side(zz, ch).start()
                    self.relay(zz * 2 + x, ch)

                @pl.when(z + j < depth)
                def _():
                    zz = z + j
                    self.take(zz * 2 + x, ch)

                    @pl.when(z > 0)
                    def _():
                        self.send_down(zz, ch).start()

                    self.send_side(zz, ch).start()
                    self.relay(zz * 2 + x, ch)

            if ready is not None:
                @pl.when(z - j + 1 >= 0)
                def _():
                    ready(z - j + 1, j == 1)

        def crossed(zz):
            block = zz * 2 + 1 - x
            for ch in range(self.chunks):
                self.take(block, ch)
                self.relay(block, ch)

        if ready is not None:
            @pl.when(z - depth + 1 >= 0)
            def _():
                ready(z - depth + 1, False)
        else:
            crossed(z)
        for j in range(1, depth):
            if ready is None:
                @pl.when(z - j >= 0)
                def _():
                    crossed(z - j)

            @pl.when(z + j < depth)
            def _():
                crossed(z + j)

    def finish(self):
        z, depth = self.z, self.depth
        for zz in range(depth):
            for ch in range(self.chunks):
                @pl.when((zz <= z) & (z + 1 < depth))
                def _():
                    self.send_up(zz, ch).wait_send()

                @pl.when((zz >= z) & (z > 0))
                def _():
                    self.send_down(zz, ch).wait_send()

                self.send_side(zz, ch).wait_send()


def gated(rows, gate, up, down):
    gate_part = jnp.dot(rows, gate[...], preferred_element_type=F32)
    upper = jnp.dot(rows, up[...], preferred_element_type=F32)
    hidden = (gate_part / (1.0 + jnp.exp(-gate_part)) * upper).astype(BF16)
    return jnp.dot(hidden, down[...], preferred_element_type=F32).astype(BF16)


CHUNKS = 2


def rotated(values, cosine, sine):
    lane = lax.broadcasted_iota(jnp.int32, values.shape, 1)
    half = ROPE // 2
    swapped = jnp.where(lane % ROPE < half, pltpu.roll(values, LANES - half, 1), pltpu.roll(values, half, 1))
    return values * cosine + swapped * sine


def layer_kernel(depth, chips, experts,
                 latent_gain_ref, gain_ref, nope_hbm, rope_hbm, latent_hbm, key_hbm, resid_hbm, ids_hbm, route_hbm, table_hbm, kup_hbm, vup_hbm, proj_hbm, eg_hbm, eu_hbm, ed_hbm, sg_hbm, su_hbm, sd_hbm,
                 out_ref,
                 nope_ref, rope_ref, latent_ref, key_ref, resid_ref, ids_ref, route_ref, table, kup, vup, proj_ref, eg, eu, ed, sg, su, sd, load_sem,
                 lat, query, heads_ref, mixed, tops, sums, l_up, l_down, l_side, l_got, relay_out, relay_in,
                 part, sib, ysend, yrecv, sib_s, sib_r, y_s, y_r,
                 hid, shared, xbuf, up, down, side, got,
                 contrib, xr, upr, dnr, rx_s, rx_r, rz_s, up_r, dn_r):
    me = lax.axis_index("sp")
    t = lax.axis_index("tp")
    z, x = me // 2, me % 2
    y, c = t // 2, t % 2
    tokens, width = resid_ref.shape
    rows, rank = latent_ref.shape
    head_cols = nope_ref.shape[1]
    local_heads = head_cols // NOPE
    columns = pl.ds(pl.multiple_of(t * head_cols, head_cols), head_cols)
    loads = [pltpu.make_async_copy(src, dst, load_sem.at[i]) for i, (src, dst) in enumerate(
        ((latent_hbm, latent_ref), (key_hbm, key_ref),
         (table_hbm.at[pl.ds(pl.multiple_of(me * rows, rows), rows)], table),
         (nope_hbm, nope_ref), (rope_hbm, rope_ref), (ids_hbm, ids_ref), (route_hbm, route_ref),
         (kup_hbm.at[:, columns], kup), (vup_hbm.at[:, columns], vup), (proj_hbm, proj_ref), (resid_hbm, resid_ref),
         (sg_hbm, sg), (su_hbm, su), (sd_hbm, sd), (eg_hbm.at[0], eg), (eu_hbm.at[0], eu), (ed_hbm.at[0], ed)))]
    for load in loads:
        load.start()
    sibling = t + 1 - 2 * c
    peers = [lax.rem(t + 2 * d, 2 * chips) for d in range(1, chips)]
    greet(z, depth, me, [sibling] + peers)

    loads[0].wait()
    wide = latent_ref[...].astype(F32)
    factor = lax.rsqrt(jnp.mean(wide * wide, axis=-1, keepdims=True) + norm_eps)
    lat[me, :, :rank] = (wide * factor * latent_gain_ref[...].astype(F32)).astype(BF16)
    loads[1].wait()
    loads[2].wait()
    cosine, sine = table[:, :ROPE], table[:, ROPE:]
    cosine = jnp.concatenate([cosine, cosine], axis=1)
    sine = jnp.concatenate([sine, sine], axis=1)
    key = key_ref[...].astype(F32).T
    lat[me, :, rank:] = rotated(jnp.concatenate([key, key], axis=1), cosine, sine).astype(BF16)

    half_rows = rows // 2

    def half_view(block, half):
        return lat.at[block, pl.ds(pl.multiple_of(half * half_rows, half_rows), half_rows)]

    def relay_copy(block):
        return pltpu.make_async_remote_copy(
            src_ref=half_view(block, c), dst_ref=half_view(block, c),
            send_sem=relay_out.at[block], recv_sem=relay_in.at[block],
            device_id={"tp": sibling}, device_id_type=MESH)

    latents = Gather(lambda b, ch: half_view(b, c), 1, l_up, l_down, l_side, l_got, z, x, depth,
                     relay=lambda b, ch: relay_copy(b).start())
    latents.start(0)
    for load in loads[3:9]:
        load.wait()
    lane = lax.broadcasted_iota(jnp.int32, (rows, LANES), 1)
    turned = rotated(rope_ref[...].astype(F32), cosine, sine)
    for h in range(local_heads):
        query[h, :, :NOPE] = nope_ref[:, h * NOPE:(h + 1) * NOPE]
        query[h, :, NOPE:] = jnp.where(lane // ROPE == h, turned, 0.0).astype(BF16)
    slot = lax.broadcasted_iota(jnp.int32, (LANES, tokens), 0)
    dense = jnp.zeros((LANES, tokens), F32)
    for k in range(ids_ref.shape[0]):
        dense = dense + jnp.where(slot % experts == ids_ref[k:k + 1, :], route_ref[k:k + 1, :], 0.0)
    coarse = dense.astype(BF16).astype(F32)
    terms = jnp.where(slot < experts, coarse, jnp.where(slot < 2 * experts, dense - coarse, 0.0))
    xbuf[me, :, width:] = terms.T.astype(BF16)
    value_t = vup[...].astype(F32).T.astype(BF16)
    vup[...] = value_t
    span = 2 * rows
    score_scale = 1.0 / math.sqrt(NOPE + ROPE)
    mixed[...] = jnp.zeros(mixed.shape, F32)
    tops[...] = jnp.full(tops.shape, -1e30, F32)
    sums[...] = jnp.zeros(sums.shape, F32)

    def attend(zz):
        pair = lat[pl.ds(zz * 2, 2)].reshape(span, rank + LANES)
        keys = jnp.dot(pair[:, :rank], kup[...], preferred_element_type=F32).astype(BF16)
        values_t = lax.dot_general(
            vup[...], pair[:, :rank], (((1,), (1,)), ((), ())), preferred_element_type=F32).astype(BF16)
        key_pos = zz * span + lax.broadcasted_iota(jnp.int32, (span, rows), 0)
        query_pos = me * rows + lax.broadcasted_iota(jnp.int32, (span, rows), 1)
        allowed = key_pos <= query_pos
        for h in range(local_heads):
            top = tops[h]
            full = jnp.concatenate([keys[:, h * NOPE:(h + 1) * NOPE], pair[:, rank:]], axis=1)
            scores = lax.dot_general(
                full, query[h], (((1,), (1,)), ((), ())), preferred_element_type=F32) * score_scale
            scores = jnp.where(allowed, scores, -1e30)
            newest = jnp.maximum(top, jnp.max(scores, axis=0, keepdims=True))
            weights = jnp.exp(scores - newest)
            shrink = jnp.exp(top - newest)
            sums[h] = sums[h] * shrink + jnp.sum(weights, axis=0, keepdims=True)
            mixed[h] = mixed[h] * shrink + jnp.dot(
                values_t[h * VDIM:(h + 1) * VDIM], weights.astype(BF16), preferred_element_type=F32)
            tops[h] = newest

    def relayed(block):
        arrived(half_view(block, 1 - c), relay_in.at[block])

    def ready(zz, own):
        across = zz * 2 + 1 - x
        latents.take(across, 0)
        relay_copy(across).start()
        if not own:
            relayed(zz * 2 + x)
        relayed(across)
        attend(zz)

    latents.run(ready)
    for h in range(local_heads):
        heads_ref[:, h * VDIM:(h + 1) * VDIM] = (mixed[h] / sums[h]).T.astype(BF16)
    loads[9].wait()
    loads[10].wait()

    def project(block):
        mine = heads_ref[pl.ds(pl.multiple_of(block * tokens, tokens), tokens), :]
        return jnp.dot(mine, proj_ref[...], preferred_element_type=F32).astype(BF16)

    piece = tokens // CHUNKS

    def to_sibling(yy, ch):
        here = pl.ds(ch * piece, piece)
        return pltpu.make_async_remote_copy(
            src_ref=part.at[yy, here], dst_ref=sib.at[yy, here], send_sem=sib_s.at[yy, ch], recv_sem=sib_r.at[yy, ch],
            device_id={"tp": sibling}, device_id_type=MESH)

    def to_chip(d, ch):
        here = pl.ds(ch * piece, piece)
        return pltpu.make_async_remote_copy(
            src_ref=ysend.at[d - 1, here], dst_ref=yrecv.at[d - 1, here],
            send_sem=y_s.at[d - 1, ch], recv_sem=y_r.at[d - 1, ch],
            device_id={"tp": peers[d - 1]}, device_id_type=MESH)

    def pair_sum(yy, mine, ch):
        here = pl.ds(ch * piece, piece)
        arrived(sib.at[yy, here], sib_r.at[yy, ch])
        return mine[ch * piece:(ch + 1) * piece] + sib[yy, here].astype(F32)

    ahead = [lax.rem(y + d, chips) for d in range(1, chips)] + [y]
    for slot, yy in enumerate(ahead):
        part[yy] = project(yy * 2 + 1 - c)
        for ch in range(CHUNKS):
            to_sibling(yy, ch).start()
        if slot < chips - 1:
            ysend[slot] = project(yy * 2 + c)
    for d in range(1, chips):
        mine = ysend[d - 1].astype(F32)
        for ch in range(CHUNKS):
            ysend[d - 1, pl.ds(ch * piece, piece)] = pair_sum(ahead[d - 1], mine, ch).astype(BF16)
            to_chip(d, ch).start()
    mine = project(y * 2 + c).astype(F32)

    ring = Gather(lambda b, ch: xbuf.at[b, pl.ds(ch * piece, piece)], CHUNKS, up, down, side, got, z, x, depth)
    for ch in range(CHUNKS):
        here = pl.ds(ch * piece, piece)
        total = pair_sum(y, mine, ch)
        for d in range(1, chips):
            arrived(yrecv.at[d - 1, here], y_r.at[d - 1, ch])
            total = total + yrecv[d - 1, here].astype(F32)
        hidden_one = (resid_ref[here].astype(F32) + total).astype(BF16)
        hid[here] = hidden_one
        wide = hidden_one.astype(F32)
        factor = lax.rsqrt(jnp.mean(wide * wide, axis=-1, keepdims=True) + norm_eps)
        xbuf[me, here, :width] = (wide * factor * gain_ref[...].astype(F32)).astype(BF16)
        ring.start(ch)
    for load in loads[11:14]:
        load.wait()
    shared[...] = gated(xbuf[me, :, :width], sg, su, sd)
    ring.run()
    for load in loads[14:]:
        load.wait()

    def cross(zz, ch):
        return pltpu.make_async_remote_copy(
            src_ref=contrib.at[zz, 1 - x, pl.ds(ch * piece, piece)], dst_ref=xr.at[zz, pl.ds(ch * piece, piece)],
            send_sem=rx_s.at[zz, ch], recv_sem=rx_r.at[zz, ch],
            device_id={"sp": z * 2 + 1 - x}, device_id_type=MESH)

    high = (z >= depth // 2).astype(jnp.int32)

    def expert_step(j, carry):
        pick = high * j + (1 - high) * (depth - 2 - j)
        pick = pick + (pick >= z).astype(jnp.int32)
        last = (j == depth - 1).astype(jnp.int32)
        zz = last * z + (1 - last) * pick
        pair = xbuf[pl.ds(zz * 2, 2)].reshape(2 * tokens, width + LANES)
        routes = pair[:, width:].astype(F32)
        lane = lax.broadcasted_iota(jnp.int32, routes.shape, 1)
        weight = jnp.sum(jnp.where((lane == me) | (lane == me + experts), routes, 0.0), axis=1, keepdims=True)
        answer = gated(pair[:, :width], eg, eu, ed).astype(F32) * weight
        contrib[zz] = answer.astype(BF16).reshape(2, tokens, width)
        for ch in range(CHUNKS):
            cross(zz, ch).start()
        return carry

    lax.fori_loop(0, depth, expert_step, 0)

    def pass_on(dst, ch, landing, recv, to):
        return pltpu.make_async_remote_copy(
            src_ref=contrib.at[dst, x, pl.ds(ch * piece, piece)], dst_ref=landing.at[dst, pl.ds(ch * piece, piece)],
            send_sem=rz_s.at[dst, ch], recv_sem=recv.at[dst, ch],
            device_id={"sp": to}, device_id_type=MESH)

    def local_sum(dst, ch):
        here = pl.ds(ch * piece, piece)
        arrived(xr.at[dst, here], rx_r.at[dst, ch])
        return contrib[dst, x, here].astype(F32) + xr[dst, here].astype(F32)

    def hop(dst, ch, landing, recv, at_end, to):
        here = pl.ds(ch * piece, piece)

        @pl.when(jnp.logical_not(at_end))
        def _():
            partial = local_sum(dst, ch)
            arrived(landing.at[dst, here], recv.at[dst, ch])
            contrib[dst, x, here] = (partial + landing[dst, here].astype(F32)).astype(BF16)

        @pl.when(at_end)
        def _():
            contrib[dst, x, here] = local_sum(dst, ch).astype(BF16)

        pass_on(dst, ch, landing, recv, to).start()

    for k in range(depth - 1):
        for ch in range(CHUNKS):
            @pl.when(depth - 1 - k > z)
            def _():
                hop(depth - 1 - k, ch, upr, up_r, z == 0, me + 2)

            @pl.when(k < z)
            def _():
                hop(k, ch, dnr, dn_r, z + 1 == depth, me - 2)

    @pl.when(z == 0)
    def _():
        upr[z] = jnp.zeros(upr.shape[1:], BF16)

    @pl.when(z + 1 == depth)
    def _():
        dnr[z] = jnp.zeros(dnr.shape[1:], BF16)

    for ch in range(CHUNKS):
        here = pl.ds(ch * piece, piece)

        @pl.when(z > 0)
        def _():
            arrived(upr.at[z, here], up_r.at[z, ch])

        @pl.when(z + 1 < depth)
        def _():
            arrived(dnr.at[z, here], dn_r.at[z, ch])

        routed = (local_sum(z, ch) + upr[z, here].astype(F32) + dnr[z, here].astype(F32)).astype(BF16)
        out_ref[here] = (hid[here].astype(F32) + routed.astype(F32) + shared[here].astype(F32)).astype(BF16)

    latents.finish()
    for zz in range(depth):
        @pl.when(zz > z)
        def _():
            relayed(zz * 2 + x)
            relayed(zz * 2 + 1 - x)

    for block in range(2 * depth):
        @pl.when(block != me)
        def _():
            relay_copy(block).wait_send()
    for ch in range(CHUNKS):
        for yy in range(chips):
            to_sibling(yy, ch).wait_send()
        for d in range(1, chips):
            to_chip(d, ch).wait_send()
    ring.finish()
    for zz in range(depth):
        for ch in range(CHUNKS):
            cross(zz, ch).wait_send()

            @pl.when(zz != z)
            def _():
                arrived(contrib.at[zz, x, pl.ds(ch * piece, piece)], rz_s.at[zz, ch])


def line_body(query_nope, query_rope, latent, key_rope, latent_gain, key_up, value_up, out_proj, residual, ffn_gain,
              expert_ids, route_weights, expert_gate, expert_up, expert_down, shared_gate, shared_up, shared_down):
    sp, tp = lax.axis_size("sp"), lax.axis_size("tp")
    depth, chips = sp // 2, tp // 2
    rows, rank = latent.shape
    tokens, width = residual.shape
    ff = shared_gate.shape[1]
    head_cols = query_nope.shape[1]
    half_dim = ROPE // 2
    frequency = np.float32(rope_base) ** (-np.arange(half_dim, dtype=np.float32) / np.float32(half_dim))
    angles = np.arange(sp * rows, dtype=np.float32)[:, None] * frequency[None, :]
    cosine, sine = np.cos(angles), np.sin(angles)
    table = jnp.asarray(np.concatenate([cosine, cosine, -sine, sine], axis=1), F32)
    dma = pltpu.SemaphoreType.DMA
    vmem = pl.BlockSpec(memory_space=pltpu.VMEM)
    hbm = pl.BlockSpec(memory_space=pl.ANY)
    block = (tokens, width)

    def buf(*shape):
        return pltpu.VMEM(shape, BF16)

    scratch = [
        buf(*query_nope.shape), buf(*query_rope.shape), buf(rows, rank), buf(ROPE, rows), buf(*block),
        pltpu.VMEM(expert_ids.shape[::-1], jnp.int32), pltpu.VMEM(expert_ids.shape[::-1], F32),
        pltpu.VMEM((rows, 2 * ROPE), F32), buf(rank, head_cols), buf(rank, head_cols), buf(head_cols, width),
        buf(width, ff), buf(width, ff), buf(ff, width), buf(width, ff), buf(width, ff), buf(ff, width), dma((17,)),
        buf(sp, rows, rank + LANES), buf(head_cols // NOPE, rows, NOPE + LANES), buf(rows, head_cols),
        pltpu.VMEM((head_cols // VDIM, VDIM, rows), F32),
        pltpu.VMEM((head_cols // NOPE, 1, rows), F32), pltpu.VMEM((head_cols // NOPE, 1, rows), F32),
        dma((depth, 1)), dma((depth, 1)), dma((depth, 1)), dma((sp, 1)), dma((sp,)), dma((sp,)),
        buf(chips, *block), buf(chips, *block), buf(chips - 1, *block), buf(chips - 1, *block),
        dma((chips, CHUNKS)), dma((chips, CHUNKS)), dma((chips - 1, CHUNKS)), dma((chips - 1, CHUNKS)),
        buf(*block), buf(*block), buf(sp, tokens, width + LANES),
        dma((depth, CHUNKS)), dma((depth, CHUNKS)), dma((depth, CHUNKS)), dma((sp, CHUNKS)),
        buf(depth, 2, *block), buf(depth, *block), buf(depth, *block), buf(depth, *block),
    ] + [dma((depth, CHUNKS))] * 5
    return pl.pallas_call(
        functools.partial(layer_kernel, depth, chips, sp),
        out_shape=jax.ShapeDtypeStruct(block, BF16),
        in_specs=[vmem] * 2 + [hbm] * 17,
        out_specs=vmem,
        scratch_shapes=scratch,
        compiler_params=pltpu.CompilerParams(
            collective_id=0, has_side_effects=True, vmem_limit_bytes=67043328),
        name="layer",
    )(latent_gain, ffn_gain, query_nope, query_rope, latent, key_rope.T, residual,
      expert_ids.T, route_weights.T, table, key_up, value_up, out_proj,
      expert_gate, expert_up, expert_down, shared_gate, shared_up, shared_down)


def body(*args):
    latent, residual, expert_ids, expert_gate = args[2], args[8], args[10], args[12]
    sp, tp = lax.axis_size("sp"), lax.axis_size("tp")
    tokens, slots = residual.shape[0], expert_ids.shape[1]
    experts = expert_gate.shape[0] * sp
    capacity = 2 * tokens * slots // experts
    dense = capacity >= tokens and expert_gate.shape[0] == 1 and args[0].shape[1] == 2 * NOPE == latent.shape[1]
    if dense and sp % 2 == 0 and tp % 2 == 0 and tp > 2 and 2 * sp <= LANES:
        return line_body(*args)
    return start_body(*args)


def solution(mesh):
    in_specs = (
        P("sp", "tp"),
        P("sp", "tp"),
        P("sp", None),
        P("sp", None),
        P(),
        P(),
        P(),
        P("tp", None),
        P(("sp", "tp"), None),
        P(),
        P(("sp", "tp"), None),
        P(("sp", "tp"), None),
        P("sp", None, None),
        P("sp", None, None),
        P("sp", None, None),
        P(),
        P(),
        P(),
    )
    out_specs = P(("sp", "tp"), None)
    return jax.shard_map(body, mesh=mesh, in_specs=in_specs, out_specs=out_specs, check_vma=False)
```

```python
import functools
import math

import jax
import jax.numpy as jnp
import numpy as np
from jax import lax
from jax.experimental import pallas as pl
from jax.experimental.pallas import tpu as pltpu
from jax.sharding import PartitionSpec as P

NOPE = 128
ROPE = 64
VDIM = 128


rope_base = 10000.0
norm_eps = 1e-06


def scale_rows(values, gain_vec):
    as_float = values.astype(jnp.float32)
    factor = lax.rsqrt(jnp.mean(as_float * as_float, axis=-1, keepdims=True) + norm_eps)
    return (as_float * factor * gain_vec.astype(jnp.float32)).astype(jnp.bfloat16)


def rotate(values, positions):
    half_dim = values.shape[-1] // 2
    frequency = rope_base ** (-jnp.arange(half_dim, dtype=jnp.float32) / half_dim)
    angles = positions.astype(jnp.float32)[:, None, None] * frequency
    cosine = jnp.cos(angles)
    sine_part = jnp.sin(angles)
    as_float = values.astype(jnp.float32)
    first_half = as_float[..., :half_dim]
    second_half = as_float[..., half_dim:]
    return jnp.concatenate(
        [
            first_half * cosine - second_half * sine_part,
            first_half * sine_part + second_half * cosine,
        ],
        axis=-1,
    ).astype(jnp.bfloat16)


def start_body(
    query_nope,
    query_rope,
    latent,
    key_rope,
    latent_gain,
    key_up,
    value_up,
    out_proj,
    residual,
    ffn_gain,
    expert_ids,
    route_weights,
    expert_gate,
    expert_up,
    expert_down,
    shared_gate,
    shared_up,
    shared_down,
):
    row_count = latent.shape[0]
    first_row = lax.axis_index("sp") * row_count
    last_row = first_row + row_count - 1
    positions = first_row + jnp.arange(row_count, dtype=jnp.int32)
    local_heads = query_nope.shape[1] // NOPE
    head_start = lax.axis_index("tp") * local_heads
    key_local = lax.dynamic_slice_in_dim(key_up, head_start * NOPE, local_heads * NOPE, 1)
    value_local = lax.dynamic_slice_in_dim(value_up, head_start * VDIM, local_heads * VDIM, 1)
    normed_latent = scale_rows(latent, latent_gain)
    rot_key = rotate(key_rope[:, None, :], positions)[:, 0, :]
    queries_nope = query_nope.reshape(row_count, local_heads, NOPE)
    rot_query = rotate(query_rope.reshape(row_count, local_heads, ROPE), positions)
    score_scale = 1.0 / math.sqrt(NOPE + ROPE)

    def expand(block_latent):
        keys_flat = jnp.dot(block_latent, key_local, preferred_element_type=jnp.float32).astype(
            jnp.bfloat16
        )
        values_flat = jnp.dot(block_latent, value_local, preferred_element_type=jnp.float32).astype(
            jnp.bfloat16
        )
        return (keys_flat, values_flat)

    def attend(state_now, keys_flat, values_flat, keys_rope, key_start):
        running, weight_sum, weighted = state_now
        key_count = keys_flat.shape[0]
        key_heads = keys_flat.reshape(key_count, local_heads, NOPE)
        value_heads = values_flat.reshape(key_count, local_heads, VDIM)
        scores = jnp.einsum(
            "qhd,khd->hqk", queries_nope, key_heads, preferred_element_type=jnp.float32
        )
        scores = (
            scores
            + jnp.einsum("qhd,kd->hqk", rot_query, keys_rope, preferred_element_type=jnp.float32)
        ) * score_scale
        key_pos = key_start + jnp.arange(key_count, dtype=jnp.int32)
        allowed = (key_pos[None, :] <= positions[:, None])[None]
        scores = jnp.where(allowed, scores, -1e30)
        newest = jnp.maximum(running, jnp.max(scores, axis=-1))
        weights = jnp.where(allowed, jnp.exp(scores - newest[..., None]), 0.0)
        shrink = jnp.exp(running - newest)
        weight_sum = weight_sum * shrink + jnp.sum(weights, axis=-1)
        mixed = jnp.einsum(
            "hqk,khd->qhd",
            weights.astype(jnp.bfloat16),
            value_heads,
            preferred_element_type=jnp.float32,
        )
        weighted = weighted * shrink.T[:, :, None] + mixed
        return (newest, weight_sum, weighted)

    initial = (
        jnp.full((local_heads, row_count), -jnp.inf, jnp.float32),
        jnp.zeros((local_heads, row_count), jnp.float32),
        jnp.zeros((row_count, local_heads, VDIM), jnp.float32),
    )
    pieces = (
        lax.all_gather(normed_latent, "sp", axis=0, tiled=True),
        lax.all_gather(rot_key, "sp", axis=0, tiled=True),
    )
    piece_len = pieces[0].shape[0]
    span_len = math.gcd(piece_len, 1024)

    def advance(step_num, state_in):
        offset = step_num * span_len
        sliced = tuple((lax.dynamic_slice_in_dim(member, offset, span_len, 0) for member in pieces))

        def compute(state_cur):
            keys_flat, values_flat = expand(sliced[0])
            return attend(state_cur, keys_flat, values_flat, sliced[-1], offset)

        def unchanged(state_cur):
            return state_cur

        return lax.cond(offset <= last_row, compute, unchanged, state_in)

    folded = lax.fori_loop(0, piece_len // span_len, advance, initial)
    heads_out = (
        (folded[2] / folded[1].T[:, :, None])
        .astype(jnp.bfloat16)
        .reshape(row_count, local_heads * VDIM)
    )
    tokens = residual.shape[0]
    attn_sum = lax.psum_scatter(
        jnp.dot(heads_out, out_proj, preferred_element_type=jnp.float32).astype(jnp.bfloat16),
        "tp",
        scatter_dimension=0,
        tiled=True,
    ).astype(jnp.float32)
    hidden_one = (residual.astype(jnp.float32) + attn_sum).astype(jnp.bfloat16)
    normed = scale_rows(hidden_one, ffn_gain)
    slot_count = expert_ids.shape[1]
    model_width = residual.shape[1]
    local_experts = expert_gate.shape[0]
    experts = local_experts * lax.axis_size("sp")
    capacity = max(2, 2 * tokens * slot_count // experts)
    flat_ids = expert_ids.reshape(-1)
    onehot = (flat_ids[:, None] == jnp.arange(experts, dtype=jnp.int32)[None, :]).astype(jnp.int32)
    slot_rank = jnp.sum(jnp.cumsum(onehot, axis=0) * onehot, axis=1) - 1
    target = flat_ids * capacity + slot_rank
    slot_token = (
        jnp.full((experts * capacity,), tokens, jnp.int32)
        .at[target]
        .set(jnp.arange(tokens * slot_count, dtype=jnp.int32) // slot_count)
    )
    padded = jnp.concatenate([normed, jnp.zeros((1, model_width), jnp.bfloat16)], axis=0)
    outgoing = padded[slot_token].reshape(experts, capacity, model_width)
    arrived = lax.all_to_all(outgoing, "sp", split_axis=0, concat_axis=0, tiled=True)
    item_count = arrived.shape[1]
    grouped = arrived.reshape(-1, local_experts, item_count, model_width)
    gate_part = jnp.einsum(
        "seid,edf->seif", grouped, expert_gate, preferred_element_type=jnp.float32
    )
    upper_part = jnp.einsum(
        "seid,edf->seif", grouped, expert_up, preferred_element_type=jnp.float32
    )
    expert_hidden = (jax.nn.silu(gate_part) * upper_part).astype(jnp.bfloat16)
    expert_rows = jnp.einsum(
        "seif,efd->seid", expert_hidden, expert_down, preferred_element_type=jnp.float32
    ).astype(jnp.bfloat16)
    answered = expert_rows.reshape(-1, item_count, model_width)
    returned = lax.all_to_all(answered, "sp", split_axis=0, concat_axis=0, tiled=True)
    picked = returned.reshape(experts * capacity, model_width)[target]
    routed = jnp.sum(
        (picked.astype(jnp.float32) * route_weights.reshape(-1)[:, None]).reshape(
            tokens, slot_count, model_width
        ),
        axis=1,
    ).astype(jnp.bfloat16)
    shared_gate_part = jnp.dot(normed, shared_gate, preferred_element_type=jnp.float32)
    shared_upper = jnp.dot(normed, shared_up, preferred_element_type=jnp.float32)
    shared_hidden = (jax.nn.silu(shared_gate_part) * shared_upper).astype(jnp.bfloat16)
    shared_rows = jnp.dot(shared_hidden, shared_down, preferred_element_type=jnp.float32).astype(
        jnp.bfloat16
    )
    return (
        hidden_one.astype(jnp.float32)
        + routed.astype(jnp.float32)
        + shared_rows.astype(jnp.float32)
    ).astype(jnp.bfloat16)


MESH = pl.DeviceIdType.MESH
F32 = jnp.float32
BF16 = jnp.bfloat16
LANES = 128


def arrived(ref, sem):
    pltpu.make_async_copy(ref, ref, sem).wait()


def greet(z, depth, me, tp_peers):
    barrier = pltpu.get_barrier_semaphore()

    @pl.when(z + 1 < depth)
    def _():
        pl.semaphore_signal(barrier, inc=1, device_id={"sp": me + 2}, device_id_type=MESH)

    @pl.when(z > 0)
    def _():
        pl.semaphore_signal(barrier, inc=1, device_id={"sp": me - 2}, device_id_type=MESH)

    pair = z * 4 + 1 - me
    pl.semaphore_signal(barrier, inc=1, device_id={"sp": pair}, device_id_type=MESH)
    for peer in tp_peers:
        pl.semaphore_signal(barrier, inc=1, device_id={"tp": peer}, device_id_type=MESH)
    line_peers = (z + 1 < depth).astype(jnp.int32) + (z > 0).astype(jnp.int32)
    pl.semaphore_wait(barrier, 1 + len(tp_peers) + line_peers)


class Gather:
    def __init__(self, view, chunks, up, down, side, got, z, x, depth, relay=None):
        self.view, self.up, self.down, self.side, self.got = view, up, down, side, got
        self.z, self.x, self.depth, self.chunks = z, x, depth, chunks
        self.relay = relay if relay is not None else (lambda block, ch: None)
        self.me = z * 2 + x

    def copy(self, block, ch, sem, to):
        return pltpu.make_async_remote_copy(
            src_ref=self.view(block, ch), dst_ref=self.view(block, ch), send_sem=sem,
            recv_sem=self.got.at[block, ch], device_id={"sp": to}, device_id_type=MESH)

    def send_up(self, zz, ch):
        return self.copy(zz * 2 + self.x, ch, self.up.at[zz, ch], self.me + 2)

    def send_down(self, zz, ch):
        return self.copy(zz * 2 + self.x, ch, self.down.at[zz, ch], self.me - 2)

    def send_side(self, zz, ch):
        return self.copy(zz * 2 + self.x, ch, self.side.at[zz, ch], self.z * 2 + 1 - self.x)

    def take(self, block, ch):
        arrived(self.view(block, ch), self.got.at[block, ch])

    def start(self, ch):
        z = self.z

        @pl.when(z + 1 < self.depth)
        def _():
            self.send_up(z, ch).start()

        @pl.when(z > 0)
        def _():
            self.send_down(z, ch).start()

        self.send_side(z, ch).start()

    def run(self, ready=None):
        z, x, depth = self.z, self.x, self.depth
        for j in range(1, depth):
            for ch in range(self.chunks):
                @pl.when(z - j >= 0)
                def _():
                    zz = z - j
                    self.take(zz * 2 + x, ch)

                    @pl.when(z + 1 < depth)
                    def _():
                        self.send_up(zz, ch).start()

                    self.send_side(zz, ch).start()
                    self.relay(zz * 2 + x, ch)

                @pl.when(z + j < depth)
                def _():
                    zz = z + j
                    self.take(zz * 2 + x, ch)

                    @pl.when(z > 0)
                    def _():
                        self.send_down(zz, ch).start()

                    self.send_side(zz, ch).start()
                    self.relay(zz * 2 + x, ch)

            if ready is not None:
                @pl.when(z - j + 1 >= 0)
                def _():
                    ready(z - j + 1, j == 1)

        def crossed(zz):
            block = zz * 2 + 1 - x
            for ch in range(self.chunks):
                self.take(block, ch)
                self.relay(block, ch)

        if ready is not None:
            @pl.when(z - depth + 1 >= 0)
            def _():
                ready(z - depth + 1, False)
        else:
            crossed(z)
        for j in range(1, depth):
            if ready is None:
                @pl.when(z - j >= 0)
                def _():
                    crossed(z - j)

            @pl.when(z + j < depth)
            def _():
                crossed(z + j)

    def finish(self):
        z, depth = self.z, self.depth
        for zz in range(depth):
            for ch in range(self.chunks):
                @pl.when((zz <= z) & (z + 1 < depth))
                def _():
                    self.send_up(zz, ch).wait_send()

                @pl.when((zz >= z) & (z > 0))
                def _():
                    self.send_down(zz, ch).wait_send()

                self.send_side(zz, ch).wait_send()


def gated(rows, gate, up, down):
    gate_part = jnp.dot(rows, gate[...], preferred_element_type=F32)
    upper = jnp.dot(rows, up[...], preferred_element_type=F32)
    hidden = (gate_part / (1.0 + jnp.exp(-gate_part)) * upper).astype(BF16)
    return jnp.dot(hidden, down[...], preferred_element_type=F32).astype(BF16)


CHUNKS = 4


def rotated(values, cosine, sine):
    lane = lax.broadcasted_iota(jnp.int32, values.shape, 1)
    half = ROPE // 2
    swapped = jnp.where(lane % ROPE < half, pltpu.roll(values, LANES - half, 1), pltpu.roll(values, half, 1))
    return values * cosine + swapped * sine


def layer_kernel(depth, chips, experts,
                 latent_gain_ref, gain_ref, nope_hbm, rope_hbm, latent_hbm, key_hbm, resid_hbm, ids_hbm, route_hbm, table_hbm, kup_hbm, vup_hbm, proj_hbm, eg_hbm, eu_hbm, ed_hbm, sg_hbm, su_hbm, sd_hbm,
                 out_ref,
                 nope_ref, rope_ref, latent_ref, key_ref, resid_ref, ids_ref, route_ref, table, kup, vup, proj_ref, eg, eu, ed, sg, su, sd, load_sem,
                 lat, query, heads_ref, mixed, tops, sums, l_up, l_down, l_side, l_got, relay_out, relay_in,
                 part, sib, ysend, yrecv, sib_s, sib_r, y_s, y_r,
                 hid, shared, xbuf, up, down, side, got,
                 contrib, xr, upr, dnr, rx_s, rx_r, rz_s, up_r, dn_r):
    me = lax.axis_index("sp")
    t = lax.axis_index("tp")
    z, x = me // 2, me % 2
    y, c = t // 2, t % 2
    tokens, width = resid_ref.shape
    rows, rank = latent_ref.shape
    head_cols = nope_ref.shape[1]
    local_heads = head_cols // NOPE
    columns = pl.ds(pl.multiple_of(t * head_cols, head_cols), head_cols)
    loads = [pltpu.make_async_copy(src, dst, load_sem.at[i]) for i, (src, dst) in enumerate(
        ((latent_hbm, latent_ref), (key_hbm, key_ref),
         (table_hbm.at[pl.ds(pl.multiple_of(me * rows, rows), rows)], table),
         (nope_hbm, nope_ref), (rope_hbm, rope_ref), (ids_hbm, ids_ref), (route_hbm, route_ref),
         (kup_hbm.at[:, columns], kup), (vup_hbm.at[:, columns], vup), (proj_hbm, proj_ref), (resid_hbm, resid_ref),
         (sg_hbm, sg), (su_hbm, su), (sd_hbm, sd), (eg_hbm.at[0], eg), (eu_hbm.at[0], eu), (ed_hbm.at[0], ed)))]
    for load in loads:
        load.start()
    sibling = t + 1 - 2 * c
    peers = [lax.rem(t + 2 * d, 2 * chips) for d in range(1, chips)]
    greet(z, depth, me, [sibling] + peers)

    loads[0].wait()
    wide = latent_ref[...].astype(F32)
    factor = lax.rsqrt(jnp.mean(wide * wide, axis=-1, keepdims=True) + norm_eps)
    lat[me, :, :rank] = (wide * factor * latent_gain_ref[...].astype(F32)).astype(BF16)
    loads[1].wait()
    loads[2].wait()
    cosine, sine = table[:, :ROPE], table[:, ROPE:]
    cosine = jnp.concatenate([cosine, cosine], axis=1)
    sine = jnp.concatenate([sine, sine], axis=1)
    key = key_ref[...].astype(F32).T
    lat[me, :, rank:] = rotated(jnp.concatenate([key, key], axis=1), cosine, sine).astype(BF16)

    half_rows = rows // 2

    def half_view(block, half):
        return lat.at[block, pl.ds(pl.multiple_of(half * half_rows, half_rows), half_rows)]

    def relay_copy(block):
        return pltpu.make_async_remote_copy(
            src_ref=half_view(block, c), dst_ref=half_view(block, c),
            send_sem=relay_out.at[block], recv_sem=relay_in.at[block],
            device_id={"tp": sibling}, device_id_type=MESH)

    latents = Gather(lambda b, ch: half_view(b, c), 1, l_up, l_down, l_side, l_got, z, x, depth,
                     relay=lambda b, ch: relay_copy(b).start())
    latents.start(0)
    for load in loads[3:9]:
        load.wait()
    lane = lax.broadcasted_iota(jnp.int32, (rows, LANES), 1)
    turned = rotated(rope_ref[...].astype(F32), cosine, sine)
    for h in range(local_heads):
        query[h, :, :NOPE] = nope_ref[:, h * NOPE:(h + 1) * NOPE]
        query[h, :, NOPE:] = jnp.where(lane // ROPE == h, turned, 0.0).astype(BF16)
    slot = lax.broadcasted_iota(jnp.int32, (LANES, tokens), 0)
    dense = jnp.zeros((LANES, tokens), F32)
    for k in range(ids_ref.shape[0]):
        dense = dense + jnp.where(slot % experts == ids_ref[k:k + 1, :], route_ref[k:k + 1, :], 0.0)
    coarse = dense.astype(BF16).astype(F32)
    terms = jnp.where(slot < experts, coarse, jnp.where(slot < 2 * experts, dense - coarse, 0.0))
    xbuf[me, :, width:] = terms.T.astype(BF16)
    value_t = vup[...].astype(F32).T.astype(BF16)
    vup[...] = value_t
    span = 2 * rows
    score_scale = 1.0 / math.sqrt(NOPE + ROPE)
    mixed[...] = jnp.zeros(mixed.shape, F32)
    tops[...] = jnp.full(tops.shape, -1e30, F32)
    sums[...] = jnp.zeros(sums.shape, F32)

    def attend(zz):
        pair = lat[pl.ds(zz * 2, 2)].reshape(span, rank + LANES)
        keys = jnp.dot(pair[:, :rank], kup[...], preferred_element_type=F32).astype(BF16)
        values_t = lax.dot_general(
            vup[...], pair[:, :rank], (((1,), (1,)), ((), ())), preferred_element_type=F32).astype(BF16)
        key_pos = zz * span + lax.broadcasted_iota(jnp.int32, (span, rows), 0)
        query_pos = me * rows + lax.broadcasted_iota(jnp.int32, (span, rows), 1)
        allowed = key_pos <= query_pos
        for h in range(local_heads):
            top = tops[h]
            full = jnp.concatenate([keys[:, h * NOPE:(h + 1) * NOPE], pair[:, rank:]], axis=1)
            scores = lax.dot_general(
                full, query[h], (((1,), (1,)), ((), ())), preferred_element_type=F32) * score_scale
            scores = jnp.where(allowed, scores, -1e30)
            newest = jnp.maximum(top, jnp.max(scores, axis=0, keepdims=True))
            weights = jnp.exp(scores - newest)
            shrink = jnp.exp(top - newest)
            sums[h] = sums[h] * shrink + jnp.sum(weights, axis=0, keepdims=True)
            mixed[h] = mixed[h] * shrink + jnp.dot(
                values_t[h * VDIM:(h + 1) * VDIM], weights.astype(BF16), preferred_element_type=F32)
            tops[h] = newest

    def relayed(block):
        arrived(half_view(block, 1 - c), relay_in.at[block])

    def ready(zz, own):
        across = zz * 2 + 1 - x
        latents.take(across, 0)
        relay_copy(across).start()
        if not own:
            relayed(zz * 2 + x)
        relayed(across)
        attend(zz)

    latents.run(ready)
    for h in range(local_heads):
        heads_ref[:, h * VDIM:(h + 1) * VDIM] = (mixed[h] / sums[h]).T.astype(BF16)
    loads[9].wait()
    loads[10].wait()

    def project(block):
        mine = heads_ref[pl.ds(pl.multiple_of(block * tokens, tokens), tokens), :]
        return jnp.dot(mine, proj_ref[...], preferred_element_type=F32).astype(BF16)

    piece = tokens // CHUNKS

    def to_sibling(yy, ch):
        here = pl.ds(ch * piece, piece)
        return pltpu.make_async_remote_copy(
            src_ref=part.at[yy, here], dst_ref=sib.at[yy, here], send_sem=sib_s.at[yy, ch], recv_sem=sib_r.at[yy, ch],
            device_id={"tp": sibling}, device_id_type=MESH)

    def to_chip(d, ch):
        here = pl.ds(ch * piece, piece)
        return pltpu.make_async_remote_copy(
            src_ref=ysend.at[d - 1, here], dst_ref=yrecv.at[d - 1, here],
            send_sem=y_s.at[d - 1, ch], recv_sem=y_r.at[d - 1, ch],
            device_id={"tp": peers[d - 1]}, device_id_type=MESH)

    def pair_sum(yy, mine, ch):
        here = pl.ds(ch * piece, piece)
        arrived(sib.at[yy, here], sib_r.at[yy, ch])
        return mine[ch * piece:(ch + 1) * piece] + sib[yy, here].astype(F32)

    ahead = [lax.rem(y + d, chips) for d in range(1, chips)] + [y]
    for slot, yy in enumerate(ahead):
        part[yy] = project(yy * 2 + 1 - c)
        for ch in range(CHUNKS):
            to_sibling(yy, ch).start()
        if slot < chips - 1:
            ysend[slot] = project(yy * 2 + c)
    for d in range(1, chips):
        mine = ysend[d - 1].astype(F32)
        for ch in range(CHUNKS):
            ysend[d - 1, pl.ds(ch * piece, piece)] = pair_sum(ahead[d - 1], mine, ch).astype(BF16)
            to_chip(d, ch).start()
    mine = project(y * 2 + c).astype(F32)

    ring = Gather(lambda b, ch: xbuf.at[b, pl.ds(ch * piece, piece)], CHUNKS, up, down, side, got, z, x, depth)
    for ch in range(CHUNKS):
        here = pl.ds(ch * piece, piece)
        total = pair_sum(y, mine, ch)
        for d in range(1, chips):
            arrived(yrecv.at[d - 1, here], y_r.at[d - 1, ch])
            total = total + yrecv[d - 1, here].astype(F32)
        hidden_one = (resid_ref[here].astype(F32) + total).astype(BF16)
        hid[here] = hidden_one
        wide = hidden_one.astype(F32)
        factor = lax.rsqrt(jnp.mean(wide * wide, axis=-1, keepdims=True) + norm_eps)
        xbuf[me, here, :width] = (wide * factor * gain_ref[...].astype(F32)).astype(BF16)
        ring.start(ch)
    for load in loads[11:14]:
        load.wait()
    shared[...] = gated(xbuf[me, :, :width], sg, su, sd)
    ring.run()
    for load in loads[14:]:
        load.wait()

    def cross(zz, ch):
        return pltpu.make_async_remote_copy(
            src_ref=contrib.at[zz, 1 - x, pl.ds(ch * piece, piece)], dst_ref=xr.at[zz, pl.ds(ch * piece, piece)],
            send_sem=rx_s.at[zz, ch], recv_sem=rx_r.at[zz, ch],
            device_id={"sp": z * 2 + 1 - x}, device_id_type=MESH)

    high = (z >= depth // 2).astype(jnp.int32)

    def expert_step(j, carry):
        pick = high * j + (1 - high) * (depth - 2 - j)
        pick = pick + (pick >= z).astype(jnp.int32)
        last = (j == depth - 1).astype(jnp.int32)
        zz = last * z + (1 - last) * pick
        pair = xbuf[pl.ds(zz * 2, 2)].reshape(2 * tokens, width + LANES)
        routes = pair[:, width:].astype(F32)
        lane = lax.broadcasted_iota(jnp.int32, routes.shape, 1)
        weight = jnp.sum(jnp.where((lane == me) | (lane == me + experts), routes, 0.0), axis=1, keepdims=True)
        answer = gated(pair[:, :width], eg, eu, ed).astype(F32) * weight
        contrib[zz] = answer.astype(BF16).reshape(2, tokens, width)
        for ch in range(CHUNKS):
            cross(zz, ch).start()
        return carry

    lax.fori_loop(0, depth, expert_step, 0)

    def pass_on(dst, ch, landing, recv, to):
        return pltpu.make_async_remote_copy(
            src_ref=contrib.at[dst, x, pl.ds(ch * piece, piece)], dst_ref=landing.at[dst, pl.ds(ch * piece, piece)],
            send_sem=rz_s.at[dst, ch], recv_sem=recv.at[dst, ch],
            device_id={"sp": to}, device_id_type=MESH)

    def local_sum(dst, ch):
        here = pl.ds(ch * piece, piece)
        arrived(xr.at[dst, here], rx_r.at[dst, ch])
        return contrib[dst, x, here].astype(F32) + xr[dst, here].astype(F32)

    def hop(dst, ch, landing, recv, at_end, to):
        here = pl.ds(ch * piece, piece)

        @pl.when(jnp.logical_not(at_end))
        def _():
            partial = local_sum(dst, ch)
            arrived(landing.at[dst, here], recv.at[dst, ch])
            contrib[dst, x, here] = (partial + landing[dst, here].astype(F32)).astype(BF16)

        @pl.when(at_end)
        def _():
            contrib[dst, x, here] = local_sum(dst, ch).astype(BF16)

        pass_on(dst, ch, landing, recv, to).start()

    for k in range(depth - 1):
        for ch in range(CHUNKS):
            @pl.when(depth - 1 - k > z)
            def _():
                hop(depth - 1 - k, ch, upr, up_r, z == 0, me + 2)

            @pl.when(k < z)
            def _():
                hop(k, ch, dnr, dn_r, z + 1 == depth, me - 2)

    @pl.when(z == 0)
    def _():
        upr[z] = jnp.zeros(upr.shape[1:], BF16)

    @pl.when(z + 1 == depth)
    def _():
        dnr[z] = jnp.zeros(dnr.shape[1:], BF16)

    for ch in range(CHUNKS):
        here = pl.ds(ch * piece, piece)

        @pl.when(z > 0)
        def _():
            arrived(upr.at[z, here], up_r.at[z, ch])

        @pl.when(z + 1 < depth)
        def _():
            arrived(dnr.at[z, here], dn_r.at[z, ch])

        routed = (local_sum(z, ch) + upr[z, here].astype(F32) + dnr[z, here].astype(F32)).astype(BF16)
        out_ref[here] = (hid[here].astype(F32) + routed.astype(F32) + shared[here].astype(F32)).astype(BF16)

    latents.finish()
    for zz in range(depth):
        @pl.when(zz > z)
        def _():
            relayed(zz * 2 + x)
            relayed(zz * 2 + 1 - x)

    for block in range(2 * depth):
        @pl.when(block != me)
        def _():
            relay_copy(block).wait_send()
    for ch in range(CHUNKS):
        for yy in range(chips):
            to_sibling(yy, ch).wait_send()
        for d in range(1, chips):
            to_chip(d, ch).wait_send()
    ring.finish()
    for zz in range(depth):
        for ch in range(CHUNKS):
            cross(zz, ch).wait_send()

            @pl.when(zz != z)
            def _():
                arrived(contrib.at[zz, x, pl.ds(ch * piece, piece)], rz_s.at[zz, ch])


def line_body(query_nope, query_rope, latent, key_rope, latent_gain, key_up, value_up, out_proj, residual, ffn_gain,
              expert_ids, route_weights, expert_gate, expert_up, expert_down, shared_gate, shared_up, shared_down):
    sp, tp = lax.axis_size("sp"), lax.axis_size("tp")
    depth, chips = sp // 2, tp // 2
    rows, rank = latent.shape
    tokens, width = residual.shape
    ff = shared_gate.shape[1]
    head_cols = query_nope.shape[1]
    half_dim = ROPE // 2
    frequency = np.float32(rope_base) ** (-np.arange(half_dim, dtype=np.float32) / np.float32(half_dim))
    angles = np.arange(sp * rows, dtype=np.float32)[:, None] * frequency[None, :]
    cosine, sine = np.cos(angles), np.sin(angles)
    table = jnp.asarray(np.concatenate([cosine, cosine, -sine, sine], axis=1), F32)
    dma = pltpu.SemaphoreType.DMA
    vmem = pl.BlockSpec(memory_space=pltpu.VMEM)
    hbm = pl.BlockSpec(memory_space=pl.ANY)
    block = (tokens, width)

    def buf(*shape):
        return pltpu.VMEM(shape, BF16)

    scratch = [
        buf(*query_nope.shape), buf(*query_rope.shape), buf(rows, rank), buf(ROPE, rows), buf(*block),
        pltpu.VMEM(expert_ids.shape[::-1], jnp.int32), pltpu.VMEM(expert_ids.shape[::-1], F32),
        pltpu.VMEM((rows, 2 * ROPE), F32), buf(rank, head_cols), buf(rank, head_cols), buf(head_cols, width),
        buf(width, ff), buf(width, ff), buf(ff, width), buf(width, ff), buf(width, ff), buf(ff, width), dma((17,)),
        buf(sp, rows, rank + LANES), buf(head_cols // NOPE, rows, NOPE + LANES), buf(rows, head_cols),
        pltpu.VMEM((head_cols // VDIM, VDIM, rows), F32),
        pltpu.VMEM((head_cols // NOPE, 1, rows), F32), pltpu.VMEM((head_cols // NOPE, 1, rows), F32),
        dma((depth, 1)), dma((depth, 1)), dma((depth, 1)), dma((sp, 1)), dma((sp,)), dma((sp,)),
        buf(chips, *block), buf(chips, *block), buf(chips - 1, *block), buf(chips - 1, *block),
        dma((chips, CHUNKS)), dma((chips, CHUNKS)), dma((chips - 1, CHUNKS)), dma((chips - 1, CHUNKS)),
        buf(*block), buf(*block), buf(sp, tokens, width + LANES),
        dma((depth, CHUNKS)), dma((depth, CHUNKS)), dma((depth, CHUNKS)), dma((sp, CHUNKS)),
        buf(depth, 2, *block), buf(depth, *block), buf(depth, *block), buf(depth, *block),
    ] + [dma((depth, CHUNKS))] * 5
    return pl.pallas_call(
        functools.partial(layer_kernel, depth, chips, sp),
        out_shape=jax.ShapeDtypeStruct(block, BF16),
        in_specs=[vmem] * 2 + [hbm] * 17,
        out_specs=vmem,
        scratch_shapes=scratch,
        compiler_params=pltpu.CompilerParams(
            collective_id=0, has_side_effects=True, vmem_limit_bytes=67043328),
        name="layer",
    )(latent_gain, ffn_gain, query_nope, query_rope, latent, key_rope.T, residual,
      expert_ids.T, route_weights.T, table, key_up, value_up, out_proj,
      expert_gate, expert_up, expert_down, shared_gate, shared_up, shared_down)


def body(*args):
    latent, residual, expert_ids, expert_gate = args[2], args[8], args[10], args[12]
    sp, tp = lax.axis_size("sp"), lax.axis_size("tp")
    tokens, slots = residual.shape[0], expert_ids.shape[1]
    experts = expert_gate.shape[0] * sp
    capacity = 2 * tokens * slots // experts
    dense = capacity >= tokens and expert_gate.shape[0] == 1 and args[0].shape[1] == 2 * NOPE == latent.shape[1]
    if dense and sp % 2 == 0 and tp % 2 == 0 and tp > 2 and 2 * sp <= LANES:
        return line_body(*args)
    return start_body(*args)


def solution(mesh):
    in_specs = (
        P("sp", "tp"),
        P("sp", "tp"),
        P("sp", None),
        P("sp", None),
        P(),
        P(),
        P(),
        P("tp", None),
        P(("sp", "tp"), None),
        P(),
        P(("sp", "tp"), None),
        P(("sp", "tp"), None),
        P("sp", None, None),
        P("sp", None, None),
        P("sp", None, None),
        P(),
        P(),
        P(),
    )
    out_specs = P(("sp", "tp"), None)
    return jax.shard_map(body, mesh=mesh, in_specs=in_specs, out_specs=out_specs, check_vma=False)
```

```python
import functools
import math

import jax
import jax.numpy as jnp
import numpy as np
from jax import lax
from jax.experimental import pallas as pl
from jax.experimental.pallas import tpu as pltpu
from jax.sharding import PartitionSpec as P

NOPE = 128
ROPE = 64
VDIM = 128


rope_base = 10000.0
norm_eps = 1e-06


def scale_rows(values, gain_vec):
    as_float = values.astype(jnp.float32)
    factor = lax.rsqrt(jnp.mean(as_float * as_float, axis=-1, keepdims=True) + norm_eps)
    return (as_float * factor * gain_vec.astype(jnp.float32)).astype(jnp.bfloat16)


def rotate(values, positions):
    half_dim = values.shape[-1] // 2
    frequency = rope_base ** (-jnp.arange(half_dim, dtype=jnp.float32) / half_dim)
    angles = positions.astype(jnp.float32)[:, None, None] * frequency
    cosine = jnp.cos(angles)
    sine_part = jnp.sin(angles)
    as_float = values.astype(jnp.float32)
    first_half = as_float[..., :half_dim]
    second_half = as_float[..., half_dim:]
    return jnp.concatenate(
        [
            first_half * cosine - second_half * sine_part,
            first_half * sine_part + second_half * cosine,
        ],
        axis=-1,
    ).astype(jnp.bfloat16)


def start_body(
    query_nope,
    query_rope,
    latent,
    key_rope,
    latent_gain,
    key_up,
    value_up,
    out_proj,
    residual,
    ffn_gain,
    expert_ids,
    route_weights,
    expert_gate,
    expert_up,
    expert_down,
    shared_gate,
    shared_up,
    shared_down,
):
    row_count = latent.shape[0]
    first_row = lax.axis_index("sp") * row_count
    last_row = first_row + row_count - 1
    positions = first_row + jnp.arange(row_count, dtype=jnp.int32)
    local_heads = query_nope.shape[1] // NOPE
    head_start = lax.axis_index("tp") * local_heads
    key_local = lax.dynamic_slice_in_dim(key_up, head_start * NOPE, local_heads * NOPE, 1)
    value_local = lax.dynamic_slice_in_dim(value_up, head_start * VDIM, local_heads * VDIM, 1)
    normed_latent = scale_rows(latent, latent_gain)
    rot_key = rotate(key_rope[:, None, :], positions)[:, 0, :]
    queries_nope = query_nope.reshape(row_count, local_heads, NOPE)
    rot_query = rotate(query_rope.reshape(row_count, local_heads, ROPE), positions)
    score_scale = 1.0 / math.sqrt(NOPE + ROPE)

    def expand(block_latent):
        keys_flat = jnp.dot(block_latent, key_local, preferred_element_type=jnp.float32).astype(
            jnp.bfloat16
        )
        values_flat = jnp.dot(block_latent, value_local, preferred_element_type=jnp.float32).astype(
            jnp.bfloat16
        )
        return (keys_flat, values_flat)

    def attend(state_now, keys_flat, values_flat, keys_rope, key_start):
        running, weight_sum, weighted = state_now
        key_count = keys_flat.shape[0]
        key_heads = keys_flat.reshape(key_count, local_heads, NOPE)
        value_heads = values_flat.reshape(key_count, local_heads, VDIM)
        scores = jnp.einsum(
            "qhd,khd->hqk", queries_nope, key_heads, preferred_element_type=jnp.float32
        )
        scores = (
            scores
            + jnp.einsum("qhd,kd->hqk", rot_query, keys_rope, preferred_element_type=jnp.float32)
        ) * score_scale
        key_pos = key_start + jnp.arange(key_count, dtype=jnp.int32)
        allowed = (key_pos[None, :] <= positions[:, None])[None]
        scores = jnp.where(allowed, scores, -1e30)
        newest = jnp.maximum(running, jnp.max(scores, axis=-1))
        weights = jnp.where(allowed, jnp.exp(scores - newest[..., None]), 0.0)
        shrink = jnp.exp(running - newest)
        weight_sum = weight_sum * shrink + jnp.sum(weights, axis=-1)
        mixed = jnp.einsum(
            "hqk,khd->qhd",
            weights.astype(jnp.bfloat16),
            value_heads,
            preferred_element_type=jnp.float32,
        )
        weighted = weighted * shrink.T[:, :, None] + mixed
        return (newest, weight_sum, weighted)

    initial = (
        jnp.full((local_heads, row_count), -jnp.inf, jnp.float32),
        jnp.zeros((local_heads, row_count), jnp.float32),
        jnp.zeros((row_count, local_heads, VDIM), jnp.float32),
    )
    pieces = (
        lax.all_gather(normed_latent, "sp", axis=0, tiled=True),
        lax.all_gather(rot_key, "sp", axis=0, tiled=True),
    )
    piece_len = pieces[0].shape[0]
    span_len = math.gcd(piece_len, 1024)

    def advance(step_num, state_in):
        offset = step_num * span_len
        sliced = tuple((lax.dynamic_slice_in_dim(member, offset, span_len, 0) for member in pieces))

        def compute(state_cur):
            keys_flat, values_flat = expand(sliced[0])
            return attend(state_cur, keys_flat, values_flat, sliced[-1], offset)

        def unchanged(state_cur):
            return state_cur

        return lax.cond(offset <= last_row, compute, unchanged, state_in)

    folded = lax.fori_loop(0, piece_len // span_len, advance, initial)
    heads_out = (
        (folded[2] / folded[1].T[:, :, None])
        .astype(jnp.bfloat16)
        .reshape(row_count, local_heads * VDIM)
    )
    tokens = residual.shape[0]
    attn_sum = lax.psum_scatter(
        jnp.dot(heads_out, out_proj, preferred_element_type=jnp.float32).astype(jnp.bfloat16),
        "tp",
        scatter_dimension=0,
        tiled=True,
    ).astype(jnp.float32)
    hidden_one = (residual.astype(jnp.float32) + attn_sum).astype(jnp.bfloat16)
    normed = scale_rows(hidden_one, ffn_gain)
    slot_count = expert_ids.shape[1]
    model_width = residual.shape[1]
    local_experts = expert_gate.shape[0]
    experts = local_experts * lax.axis_size("sp")
    capacity = max(2, 2 * tokens * slot_count // experts)
    flat_ids = expert_ids.reshape(-1)
    onehot = (flat_ids[:, None] == jnp.arange(experts, dtype=jnp.int32)[None, :]).astype(jnp.int32)
    slot_rank = jnp.sum(jnp.cumsum(onehot, axis=0) * onehot, axis=1) - 1
    target = flat_ids * capacity + slot_rank
    slot_token = (
        jnp.full((experts * capacity,), tokens, jnp.int32)
        .at[target]
        .set(jnp.arange(tokens * slot_count, dtype=jnp.int32) // slot_count)
    )
    padded = jnp.concatenate([normed, jnp.zeros((1, model_width), jnp.bfloat16)], axis=0)
    outgoing = padded[slot_token].reshape(experts, capacity, model_width)
    arrived = lax.all_to_all(outgoing, "sp", split_axis=0, concat_axis=0, tiled=True)
    item_count = arrived.shape[1]
    grouped = arrived.reshape(-1, local_experts, item_count, model_width)
    gate_part = jnp.einsum(
        "seid,edf->seif", grouped, expert_gate, preferred_element_type=jnp.float32
    )
    upper_part = jnp.einsum(
        "seid,edf->seif", grouped, expert_up, preferred_element_type=jnp.float32
    )
    expert_hidden = (jax.nn.silu(gate_part) * upper_part).astype(jnp.bfloat16)
    expert_rows = jnp.einsum(
        "seif,efd->seid", expert_hidden, expert_down, preferred_element_type=jnp.float32
    ).astype(jnp.bfloat16)
    answered = expert_rows.reshape(-1, item_count, model_width)
    returned = lax.all_to_all(answered, "sp", split_axis=0, concat_axis=0, tiled=True)
    picked = returned.reshape(experts * capacity, model_width)[target]
    routed = jnp.sum(
        (picked.astype(jnp.float32) * route_weights.reshape(-1)[:, None]).reshape(
            tokens, slot_count, model_width
        ),
        axis=1,
    ).astype(jnp.bfloat16)
    shared_gate_part = jnp.dot(normed, shared_gate, preferred_element_type=jnp.float32)
    shared_upper = jnp.dot(normed, shared_up, preferred_element_type=jnp.float32)
    shared_hidden = (jax.nn.silu(shared_gate_part) * shared_upper).astype(jnp.bfloat16)
    shared_rows = jnp.dot(shared_hidden, shared_down, preferred_element_type=jnp.float32).astype(
        jnp.bfloat16
    )
    return (
        hidden_one.astype(jnp.float32)
        + routed.astype(jnp.float32)
        + shared_rows.astype(jnp.float32)
    ).astype(jnp.bfloat16)


MESH = pl.DeviceIdType.MESH
F32 = jnp.float32
BF16 = jnp.bfloat16
LANES = 128


def arrived(ref, sem):
    pltpu.make_async_copy(ref, ref, sem).wait()


def greet(z, depth, me, tp_peers):
    barrier = pltpu.get_barrier_semaphore()

    @pl.when(z + 1 < depth)
    def _():
        pl.semaphore_signal(barrier, inc=1, device_id={"sp": me + 2}, device_id_type=MESH)

    @pl.when(z > 0)
    def _():
        pl.semaphore_signal(barrier, inc=1, device_id={"sp": me - 2}, device_id_type=MESH)

    pair = z * 4 + 1 - me
    pl.semaphore_signal(barrier, inc=1, device_id={"sp": pair}, device_id_type=MESH)
    for peer in tp_peers:
        pl.semaphore_signal(barrier, inc=1, device_id={"tp": peer}, device_id_type=MESH)
    line_peers = (z + 1 < depth).astype(jnp.int32) + (z > 0).astype(jnp.int32)
    pl.semaphore_wait(barrier, 1 + len(tp_peers) + line_peers)


class Gather:
    def __init__(self, view, whole, chunks, up, down, side, got, z, x, depth, relay=None):
        self.view, self.up, self.down, self.side, self.got = view, up, down, side, got
        self.whole = whole
        self.z, self.x, self.depth, self.chunks = z, x, depth, chunks
        self.relay = relay if relay is not None else (lambda block, ch: None)
        self.me = z * 2 + x

    def copy(self, block, ch, sem, to):
        return pltpu.make_async_remote_copy(
            src_ref=self.view(block, ch), dst_ref=self.view(block, ch), send_sem=sem,
            recv_sem=self.got.at[block, ch], device_id={"sp": to}, device_id_type=MESH)

    def send_up(self, zz, ch):
        return self.copy(zz * 2 + self.x, ch, self.up.at[zz, ch], self.me + 2)

    def send_down(self, zz, ch):
        return self.copy(zz * 2 + self.x, ch, self.down.at[zz, ch], self.me - 2)

    def send_side(self, zz):
        block = zz * 2 + self.x
        return pltpu.make_async_remote_copy(
            src_ref=self.whole(block), dst_ref=self.whole(block), send_sem=self.side.at[zz, 0],
            recv_sem=self.got.at[block, 0], device_id={"sp": self.z * 2 + 1 - self.x}, device_id_type=MESH)

    def take_side(self, block):
        arrived(self.whole(block), self.got.at[block, 0])

    def take(self, block, ch):
        arrived(self.view(block, ch), self.got.at[block, ch])

    def start(self, ch):
        z = self.z

        @pl.when(z + 1 < self.depth)
        def _():
            self.send_up(z, ch).start()

        @pl.when(z > 0)
        def _():
            self.send_down(z, ch).start()

        if ch == self.chunks - 1:
            self.send_side(z).start()

    def run(self, ready=None):
        z, x, depth = self.z, self.x, self.depth
        for j in range(1, depth):
            for ch in range(self.chunks):
                @pl.when(z - j >= 0)
                def _():
                    zz = z - j
                    self.take(zz * 2 + x, ch)

                    @pl.when(z + 1 < depth)
                    def _():
                        self.send_up(zz, ch).start()

                    if ch == self.chunks - 1:
                        self.send_side(zz).start()
                    self.relay(zz * 2 + x, ch)

                @pl.when(z + j < depth)
                def _():
                    zz = z + j
                    self.take(zz * 2 + x, ch)

                    @pl.when(z > 0)
                    def _():
                        self.send_down(zz, ch).start()

                    if ch == self.chunks - 1:
                        self.send_side(zz).start()
                    self.relay(zz * 2 + x, ch)

            if ready is not None:
                @pl.when(z - j + 1 >= 0)
                def _():
                    ready(z - j + 1, j == 1)

        def crossed(zz):
            block = zz * 2 + 1 - x
            self.take_side(block)
            self.relay(block, 0)

        if ready is not None:
            @pl.when(z - depth + 1 >= 0)
            def _():
                ready(z - depth + 1, False)
        else:
            crossed(z)
        for j in range(1, depth):
            if ready is None:
                @pl.when(z - j >= 0)
                def _():
                    crossed(z - j)

            @pl.when(z + j < depth)
            def _():
                crossed(z + j)

    def finish(self):
        z, depth = self.z, self.depth
        for zz in range(depth):
            for ch in range(self.chunks):
                @pl.when((zz <= z) & (z + 1 < depth))
                def _():
                    self.send_up(zz, ch).wait_send()

                @pl.when((zz >= z) & (z > 0))
                def _():
                    self.send_down(zz, ch).wait_send()

            self.send_side(zz).wait_send()


def gated(rows, gate, up, down):
    gate_part = jnp.dot(rows, gate[...], preferred_element_type=F32)
    upper = jnp.dot(rows, up[...], preferred_element_type=F32)
    hidden = (gate_part / (1.0 + jnp.exp(-gate_part)) * upper).astype(BF16)
    return jnp.dot(hidden, down[...], preferred_element_type=F32).astype(BF16)


CHUNKS = 2


def rotated(values, cosine, sine):
    lane = lax.broadcasted_iota(jnp.int32, values.shape, 1)
    half = ROPE // 2
    swapped = jnp.where(lane % ROPE < half, pltpu.roll(values, LANES - half, 1), pltpu.roll(values, half, 1))
    return values * cosine + swapped * sine


def layer_kernel(depth, chips, experts,
                 latent_gain_ref, gain_ref, nope_hbm, rope_hbm, latent_hbm, key_hbm, resid_hbm, ids_hbm, route_hbm, table_hbm, kup_hbm, vup_hbm, proj_hbm, eg_hbm, eu_hbm, ed_hbm, sg_hbm, su_hbm, sd_hbm,
                 out_ref,
                 nope_ref, rope_ref, latent_ref, key_ref, resid_ref, ids_ref, route_ref, table, kup, vup, proj_ref, eg, eu, ed, sg, su, sd, load_sem,
                 lat, query, heads_ref, mixed, tops, sums, l_up, l_down, l_side, l_got, relay_out, relay_in,
                 part, sib, ysend, yrecv, sib_s, sib_r, y_s, y_r,
                 hid, shared, xbuf, up, down, side, got,
                 contrib, xr, upr, dnr, rx_s, rx_r, rz_s, up_r, dn_r):
    me = lax.axis_index("sp")
    t = lax.axis_index("tp")
    z, x = me // 2, me % 2
    y, c = t // 2, t % 2
    tokens, width = resid_ref.shape
    rows, rank = latent_ref.shape
    head_cols = nope_ref.shape[1]
    local_heads = head_cols // NOPE
    columns = pl.ds(pl.multiple_of(t * head_cols, head_cols), head_cols)
    loads = [pltpu.make_async_copy(src, dst, load_sem.at[i]) for i, (src, dst) in enumerate(
        ((latent_hbm, latent_ref), (key_hbm, key_ref),
         (table_hbm.at[pl.ds(pl.multiple_of(me * rows, rows), rows)], table),
         (nope_hbm, nope_ref), (rope_hbm, rope_ref), (ids_hbm, ids_ref), (route_hbm, route_ref),
         (kup_hbm.at[:, columns], kup), (vup_hbm.at[:, columns], vup), (proj_hbm, proj_ref), (resid_hbm, resid_ref),
         (sg_hbm, sg), (su_hbm, su), (sd_hbm, sd), (eg_hbm.at[0], eg), (eu_hbm.at[0], eu), (ed_hbm.at[0], ed)))]
    for load in loads:
        load.start()
    sibling = t + 1 - 2 * c
    peers = [lax.rem(t + 2 * d, 2 * chips) for d in range(1, chips)]
    greet(z, depth, me, [sibling] + peers)

    loads[0].wait()
    wide = latent_ref[...].astype(F32)
    factor = lax.rsqrt(jnp.mean(wide * wide, axis=-1, keepdims=True) + norm_eps)
    lat[me, :, :rank] = (wide * factor * latent_gain_ref[...].astype(F32)).astype(BF16)
    loads[1].wait()
    loads[2].wait()
    cosine, sine = table[:, :ROPE], table[:, ROPE:]
    cosine = jnp.concatenate([cosine, cosine], axis=1)
    sine = jnp.concatenate([sine, sine], axis=1)
    key = key_ref[...].astype(F32).T
    lat[me, :, rank:] = rotated(jnp.concatenate([key, key], axis=1), cosine, sine).astype(BF16)

    half_rows = rows // 2

    def half_view(block, half):
        return lat.at[block, pl.ds(pl.multiple_of(half * half_rows, half_rows), half_rows)]

    def relay_copy(block):
        return pltpu.make_async_remote_copy(
            src_ref=half_view(block, c), dst_ref=half_view(block, c),
            send_sem=relay_out.at[block], recv_sem=relay_in.at[block],
            device_id={"tp": sibling}, device_id_type=MESH)

    latents = Gather(lambda b, ch: half_view(b, c), lambda b: half_view(b, c), 1, l_up, l_down, l_side, l_got, z, x, depth,
                     relay=lambda b, ch: relay_copy(b).start())
    latents.start(0)
    for load in loads[3:9]:
        load.wait()
    lane = lax.broadcasted_iota(jnp.int32, (rows, LANES), 1)
    turned = rotated(rope_ref[...].astype(F32), cosine, sine)
    for h in range(local_heads):
        query[h, :, :NOPE] = nope_ref[:, h * NOPE:(h + 1) * NOPE]
        query[h, :, NOPE:] = jnp.where(lane // ROPE == h, turned, 0.0).astype(BF16)
    slot = lax.broadcasted_iota(jnp.int32, (LANES, tokens), 0)
    dense = jnp.zeros((LANES, tokens), F32)
    for k in range(ids_ref.shape[0]):
        dense = dense + jnp.where(slot % experts == ids_ref[k:k + 1, :], route_ref[k:k + 1, :], 0.0)
    coarse = dense.astype(BF16).astype(F32)
    terms = jnp.where(slot < experts, coarse, jnp.where(slot < 2 * experts, dense - coarse, 0.0))
    xbuf[me, :, width:] = terms.T.astype(BF16)
    value_t = vup[...].astype(F32).T.astype(BF16)
    vup[...] = value_t
    span = 2 * rows
    score_scale = 1.0 / math.sqrt(NOPE + ROPE)
    mixed[...] = jnp.zeros(mixed.shape, F32)
    tops[...] = jnp.full(tops.shape, -1e30, F32)
    sums[...] = jnp.zeros(sums.shape, F32)

    def attend(zz):
        pair = lat[pl.ds(zz * 2, 2)].reshape(span, rank + LANES)
        keys = jnp.dot(pair[:, :rank], kup[...], preferred_element_type=F32).astype(BF16)
        values_t = lax.dot_general(
            vup[...], pair[:, :rank], (((1,), (1,)), ((), ())), preferred_element_type=F32).astype(BF16)
        key_pos = zz * span + lax.broadcasted_iota(jnp.int32, (span, rows), 0)
        query_pos = me * rows + lax.broadcasted_iota(jnp.int32, (span, rows), 1)
        allowed = key_pos <= query_pos
        for h in range(local_heads):
            top = tops[h]
            full = jnp.concatenate([keys[:, h * NOPE:(h + 1) * NOPE], pair[:, rank:]], axis=1)
            scores = lax.dot_general(
                full, query[h], (((1,), (1,)), ((), ())), preferred_element_type=F32) * score_scale
            scores = jnp.where(allowed, scores, -1e30)
            newest = jnp.maximum(top, jnp.max(scores, axis=0, keepdims=True))
            weights = jnp.exp(scores - newest)
            shrink = jnp.exp(top - newest)
            sums[h] = sums[h] * shrink + jnp.sum(weights, axis=0, keepdims=True)
            mixed[h] = mixed[h] * shrink + jnp.dot(
                values_t[h * VDIM:(h + 1) * VDIM], weights.astype(BF16), preferred_element_type=F32)
            tops[h] = newest

    def relayed(block):
        arrived(half_view(block, 1 - c), relay_in.at[block])

    def ready(zz, own):
        across = zz * 2 + 1 - x
        latents.take_side(across)
        relay_copy(across).start()
        if not own:
            relayed(zz * 2 + x)
        relayed(across)
        attend(zz)

    latents.run(ready)
    for h in range(local_heads):
        heads_ref[:, h * VDIM:(h + 1) * VDIM] = (mixed[h] / sums[h]).T.astype(BF16)
    loads[9].wait()
    loads[10].wait()

    def project(block):
        mine = heads_ref[pl.ds(pl.multiple_of(block * tokens, tokens), tokens), :]
        return jnp.dot(mine, proj_ref[...], preferred_element_type=F32).astype(BF16)

    piece = tokens // CHUNKS

    def to_sibling(yy, ch):
        here = pl.ds(ch * piece, piece)
        return pltpu.make_async_remote_copy(
            src_ref=part.at[yy, here], dst_ref=sib.at[yy, here], send_sem=sib_s.at[yy, ch], recv_sem=sib_r.at[yy, ch],
            device_id={"tp": sibling}, device_id_type=MESH)

    def to_chip(d, ch):
        here = pl.ds(ch * piece, piece)
        return pltpu.make_async_remote_copy(
            src_ref=ysend.at[d - 1, here], dst_ref=yrecv.at[d - 1, here],
            send_sem=y_s.at[d - 1, ch], recv_sem=y_r.at[d - 1, ch],
            device_id={"tp": peers[d - 1]}, device_id_type=MESH)

    def pair_sum(yy, mine, ch):
        here = pl.ds(ch * piece, piece)
        arrived(sib.at[yy, here], sib_r.at[yy, ch])
        return mine[ch * piece:(ch + 1) * piece] + sib[yy, here].astype(F32)

    ahead = [lax.rem(y + d, chips) for d in range(1, chips)] + [y]
    for slot, yy in enumerate(ahead):
        part[yy] = project(yy * 2 + 1 - c)
        for ch in range(CHUNKS):
            to_sibling(yy, ch).start()
        if slot < chips - 1:
            ysend[slot] = project(yy * 2 + c)
    for d in range(1, chips):
        mine = ysend[d - 1].astype(F32)
        for ch in range(CHUNKS):
            ysend[d - 1, pl.ds(ch * piece, piece)] = pair_sum(ahead[d - 1], mine, ch).astype(BF16)
            to_chip(d, ch).start()
    mine = project(y * 2 + c).astype(F32)

    ring = Gather(lambda b, ch: xbuf.at[b, pl.ds(ch * piece, piece)], lambda b: xbuf.at[b], CHUNKS,
                  up, down, side, got, z, x, depth)
    for ch in range(CHUNKS):
        here = pl.ds(ch * piece, piece)
        total = pair_sum(y, mine, ch)
        for d in range(1, chips):
            arrived(yrecv.at[d - 1, here], y_r.at[d - 1, ch])
            total = total + yrecv[d - 1, here].astype(F32)
        hidden_one = (resid_ref[here].astype(F32) + total).astype(BF16)
        hid[here] = hidden_one
        wide = hidden_one.astype(F32)
        factor = lax.rsqrt(jnp.mean(wide * wide, axis=-1, keepdims=True) + norm_eps)
        xbuf[me, here, :width] = (wide * factor * gain_ref[...].astype(F32)).astype(BF16)
        ring.start(ch)
    for load in loads[11:14]:
        load.wait()
    shared[...] = gated(xbuf[me, :, :width], sg, su, sd)
    ring.run()
    for load in loads[14:]:
        load.wait()

    def cross(zz):
        return pltpu.make_async_remote_copy(
            src_ref=contrib.at[zz, 1 - x], dst_ref=xr.at[zz],
            send_sem=rx_s.at[zz, 0], recv_sem=rx_r.at[zz, 0],
            device_id={"sp": z * 2 + 1 - x}, device_id_type=MESH)

    high = (z >= depth // 2).astype(jnp.int32)

    def expert_step(j, carry):
        pick = high * j + (1 - high) * (depth - 2 - j)
        pick = pick + (pick >= z).astype(jnp.int32)
        last = (j == depth - 1).astype(jnp.int32)
        zz = last * z + (1 - last) * pick
        pair = xbuf[pl.ds(zz * 2, 2)].reshape(2 * tokens, width + LANES)
        routes = pair[:, width:].astype(F32)
        lane = lax.broadcasted_iota(jnp.int32, routes.shape, 1)
        weight = jnp.sum(jnp.where((lane == me) | (lane == me + experts), routes, 0.0), axis=1, keepdims=True)
        answer = gated(pair[:, :width], eg, eu, ed).astype(F32) * weight
        contrib[zz] = answer.astype(BF16).reshape(2, tokens, width)
        cross(zz).start()
        return carry

    lax.fori_loop(0, depth, expert_step, 0)

    def pass_on(dst, ch, landing, recv, to):
        return pltpu.make_async_remote_copy(
            src_ref=contrib.at[dst, x, pl.ds(ch * piece, piece)], dst_ref=landing.at[dst, pl.ds(ch * piece, piece)],
            send_sem=rz_s.at[dst, ch], recv_sem=recv.at[dst, ch],
            device_id={"sp": to}, device_id_type=MESH)

    def local_sum(dst, ch):
        here = pl.ds(ch * piece, piece)
        if ch == 0:
            arrived(xr.at[dst], rx_r.at[dst, 0])
        return contrib[dst, x, here].astype(F32) + xr[dst, here].astype(F32)

    def hop(dst, ch, landing, recv, at_end, to):
        here = pl.ds(ch * piece, piece)

        @pl.when(jnp.logical_not(at_end))
        def _():
            partial = local_sum(dst, ch)
            arrived(landing.at[dst, here], recv.at[dst, ch])
            contrib[dst, x, here] = (partial + landing[dst, here].astype(F32)).astype(BF16)

        @pl.when(at_end)
        def _():
            contrib[dst, x, here] = local_sum(dst, ch).astype(BF16)

        pass_on(dst, ch, landing, recv, to).start()

    for k in range(depth - 1):
        for ch in range(CHUNKS):
            @pl.when(depth - 1 - k > z)
            def _():
                hop(depth - 1 - k, ch, upr, up_r, z == 0, me + 2)

            @pl.when(k < z)
            def _():
                hop(k, ch, dnr, dn_r, z + 1 == depth, me - 2)

    @pl.when(z == 0)
    def _():
        upr[z] = jnp.zeros(upr.shape[1:], BF16)

    @pl.when(z + 1 == depth)
    def _():
        dnr[z] = jnp.zeros(dnr.shape[1:], BF16)

    for ch in range(CHUNKS):
        here = pl.ds(ch * piece, piece)

        @pl.when(z > 0)
        def _():
            arrived(upr.at[z, here], up_r.at[z, ch])

        @pl.when(z + 1 < depth)
        def _():
            arrived(dnr.at[z, here], dn_r.at[z, ch])

        routed = (local_sum(z, ch) + upr[z, here].astype(F32) + dnr[z, here].astype(F32)).astype(BF16)
        out_ref[here] = (hid[here].astype(F32) + routed.astype(F32) + shared[here].astype(F32)).astype(BF16)

    latents.finish()
    for zz in range(depth):
        @pl.when(zz > z)
        def _():
            relayed(zz * 2 + x)
            relayed(zz * 2 + 1 - x)

    for block in range(2 * depth):
        @pl.when(block != me)
        def _():
            relay_copy(block).wait_send()
    for ch in range(CHUNKS):
        for yy in range(chips):
            to_sibling(yy, ch).wait_send()
        for d in range(1, chips):
            to_chip(d, ch).wait_send()
    ring.finish()
    for zz in range(depth):
        cross(zz).wait_send()
        for ch in range(CHUNKS):
            @pl.when(zz != z)
            def _():
                arrived(contrib.at[zz, x, pl.ds(ch * piece, piece)], rz_s.at[zz, ch])


def line_body(query_nope, query_rope, latent, key_rope, latent_gain, key_up, value_up, out_proj, residual, ffn_gain,
              expert_ids, route_weights, expert_gate, expert_up, expert_down, shared_gate, shared_up, shared_down):
    sp, tp = lax.axis_size("sp"), lax.axis_size("tp")
    depth, chips = sp // 2, tp // 2
    rows, rank = latent.shape
    tokens, width = residual.shape
    ff = shared_gate.shape[1]
    head_cols = query_nope.shape[1]
    half_dim = ROPE // 2
    frequency = np.float32(rope_base) ** (-np.arange(half_dim, dtype=np.float32) / np.float32(half_dim))
    angles = np.arange(sp * rows, dtype=np.float32)[:, None] * frequency[None, :]
    cosine, sine = np.cos(angles), np.sin(angles)
    table = jnp.asarray(np.concatenate([cosine, cosine, -sine, sine], axis=1), F32)
    dma = pltpu.SemaphoreType.DMA
    vmem = pl.BlockSpec(memory_space=pltpu.VMEM)
    hbm = pl.BlockSpec(memory_space=pl.ANY)
    block = (tokens, width)

    def buf(*shape):
        return pltpu.VMEM(shape, BF16)

    scratch = [
        buf(*query_nope.shape), buf(*query_rope.shape), buf(rows, rank), buf(ROPE, rows), buf(*block),
        pltpu.VMEM(expert_ids.shape[::-1], jnp.int32), pltpu.VMEM(expert_ids.shape[::-1], F32),
        pltpu.VMEM((rows, 2 * ROPE), F32), buf(rank, head_cols), buf(rank, head_cols), buf(head_cols, width),
        buf(width, ff), buf(width, ff), buf(ff, width), buf(width, ff), buf(width, ff), buf(ff, width), dma((17,)),
        buf(sp, rows, rank + LANES), buf(head_cols // NOPE, rows, NOPE + LANES), buf(rows, head_cols),
        pltpu.VMEM((head_cols // VDIM, VDIM, rows), F32),
        pltpu.VMEM((head_cols // NOPE, 1, rows), F32), pltpu.VMEM((head_cols // NOPE, 1, rows), F32),
        dma((depth, 1)), dma((depth, 1)), dma((depth, 1)), dma((sp, 1)), dma((sp,)), dma((sp,)),
        buf(chips, *block), buf(chips, *block), buf(chips - 1, *block), buf(chips - 1, *block),
        dma((chips, CHUNKS)), dma((chips, CHUNKS)), dma((chips - 1, CHUNKS)), dma((chips - 1, CHUNKS)),
        buf(*block), buf(*block), buf(sp, tokens, width + LANES),
        dma((depth, CHUNKS)), dma((depth, CHUNKS)), dma((depth, CHUNKS)), dma((sp, CHUNKS)),
        buf(depth, 2, *block), buf(depth, *block), buf(depth, *block), buf(depth, *block),
    ] + [dma((depth, CHUNKS))] * 5
    return pl.pallas_call(
        functools.partial(layer_kernel, depth, chips, sp),
        out_shape=jax.ShapeDtypeStruct(block, BF16),
        in_specs=[vmem] * 2 + [hbm] * 17,
        out_specs=vmem,
        scratch_shapes=scratch,
        compiler_params=pltpu.CompilerParams(
            collective_id=0, has_side_effects=True, vmem_limit_bytes=67043328),
        name="layer",
    )(latent_gain, ffn_gain, query_nope, query_rope, latent, key_rope.T, residual,
      expert_ids.T, route_weights.T, table, key_up, value_up, out_proj,
      expert_gate, expert_up, expert_down, shared_gate, shared_up, shared_down)


def body(*args):
    latent, residual, expert_ids, expert_gate = args[2], args[8], args[10], args[12]
    sp, tp = lax.axis_size("sp"), lax.axis_size("tp")
    tokens, slots = residual.shape[0], expert_ids.shape[1]
    experts = expert_gate.shape[0] * sp
    capacity = 2 * tokens * slots // experts
    dense = capacity >= tokens and expert_gate.shape[0] == 1 and args[0].shape[1] == 2 * NOPE == latent.shape[1]
    if dense and sp % 2 == 0 and tp % 2 == 0 and tp > 2 and 2 * sp <= LANES:
        return line_body(*args)
    return start_body(*args)


def solution(mesh):
    in_specs = (
        P("sp", "tp"),
        P("sp", "tp"),
        P("sp", None),
        P("sp", None),
        P(),
        P(),
        P(),
        P("tp", None),
        P(("sp", "tp"), None),
        P(),
        P(("sp", "tp"), None),
        P(("sp", "tp"), None),
        P("sp", None, None),
        P("sp", None, None),
        P("sp", None, None),
        P(),
        P(),
        P(),
    )
    out_specs = P(("sp", "tp"), None)
    return jax.shard_map(body, mesh=mesh, in_specs=in_specs, out_specs=out_specs, check_vma=False)
```
